256 devices in a mesh: ep: 64 (over z, y, core), tp: 4 (over x).
Axes of the slice: x: 4, y: 4, z: 8, core: 2. Of those that a mesh axis runs over, the one named last changes fastest.
Arguments:
- queries_a: bfloat16 [8192, 1024], P('ep', 'tp'), may hold values from -128 to 128
- queries_b: bfloat16 [8192, 1024], P('ep', 'tp'), may hold values from -128 to 128
- keys_a: bfloat16 [8192, 512], P('ep', 'tp'), may hold values from -8 to 8
- keys_b: bfloat16 [8192, 512], P('ep', 'tp'), may hold values from -8 to 8
- values: bfloat16 [8192, 1024], P('ep', 'tp'), may hold values from -6 to 6
- lambdas: float32 [16], P('tp'), may hold values from 0.3 to 0.8
- head_gain: float32 [128], replicated, may hold values from 0.1 to 1.9
- w_out: bfloat16 [2048, 2048], P('tp'), may hold values from -0.125 to 0.125
- moe_tokens: bfloat16 [32768, 2048], P(('ep', 'tp')), may hold values from -80 to 80
- moe_gain: float32 [2048], replicated, may hold values from 0.1 to 1.9
- routes: int32 [32768, 2], P(('ep', 'tp')), may hold values from 0 to 63, all different within a row; in each aligned block of 128 rows (0 to 127, 128 to 255, ...) at most 6 rows name the same one
- route_weights: float32 [32768, 2], P(('ep', 'tp')), may hold values from 0.1 to 1
- w_gate: bfloat16 [64, 2048, 2048], P('ep', None, 'tp'), may hold values from -4 to 4
- w_up: bfloat16 [64, 2048, 2048], P('ep', None, 'tp'), may hold values from -4 to 4
- w_down: bfloat16 [64, 2048, 2048], P('ep', 'tp'), may hold values from -0.0625 to 0.0625
Outputs:
- mixer_out: bfloat16 [8192, 2048], P(('ep', 'tp'))
- moe_out: bfloat16 [32768, 2048], P(('ep', 'tp'))
The draws below stay inside these ranges and needn't reach their ends.
Inputs may be any that keep to these rules, and one draw needn't show every extreme that they name: `routes`: each row names 2 different experts. Within the rows of one device no expert is named by more than 6 rows, a bound that some block reaches of some device.
All inputs are finite; a program needn't handle non-finite values.
Results may differ from the reference program's by a relative error of at most 0.011.
Values may be sent and summed in bfloat16 or wider, within the bound.
A program may use at most 192 MiB of HBM per device.

```python
import math
import jax
import jax.numpy as jnp
import numpy as np
from jax import lax

D = 2048
HEADS = 16
KV_HEADS = 8
HEAD = 64
VDIM = 128
FF = 2048
TOP = 2
ATT_DEV = 128
TOKB = 128
EXPERTS = 64
CAP = 6
SEQ = 8192
MOE_TOK = 32768
N_EP = 64
N_TP = 4


def query_key_pair(key, which):
    streams = jax.random.split(jax.random.fold_in(key, 1000 + which), 2)
    queries = 1.3 * jnp.clip(jax.random.normal(streams[0], (SEQ, HEADS * HEAD), jnp.float32), -4.0, 4.0)
    keys = 1.3 * jnp.clip(jax.random.normal(streams[1], (SEQ, KV_HEADS * HEAD), jnp.float32), -4.0, 4.0)
    return (queries, keys)


def draw_queries_a(key, part):
    return query_key_pair(key, 0)[0].astype(jnp.bfloat16)


def draw_keys_a(key, part):
    return query_key_pair(key, 0)[1].astype(jnp.bfloat16)


def draw_queries_b(key, part):
    return query_key_pair(key, 1)[0].astype(jnp.bfloat16)


def draw_keys_b(key, part):
    return query_key_pair(key, 1)[1].astype(jnp.bfloat16)


def draw_moe_tokens(key, part):
    streams = jax.random.split(jax.random.fold_in(key, 2000), 3)
    base = jnp.clip(jax.random.normal(streams[0], (MOE_TOK, D), jnp.float32), -4.0, 4.0)
    row_scale = jnp.exp(jax.random.uniform(streams[1], (MOE_TOK, 1), jnp.float32, math.log(0.3), math.log(3.0)))
    column_scale = jnp.exp(jax.random.uniform(streams[2], (1, D), jnp.float32, math.log(0.3), math.log(3.0)))
    result = base * row_scale * column_scale
    return result.astype(jnp.bfloat16)


def expert_matrix(key, salt):
    streams = jax.random.split(jax.random.fold_in(key, salt), 2)
    base = jnp.clip(jax.random.normal(streams[0], (EXPERTS, D, FF), jnp.float32), -4.0, 4.0) / math.sqrt(D)
    spread = jax.random.uniform(streams[1], (EXPERTS, 1, FF), jnp.float32, math.log(0.3), math.log(4.0))
    return (base * jnp.exp(spread)).astype(jnp.bfloat16)


def draw_w_gate(key, part):
    return expert_matrix(key, 3000)


def draw_w_up(key, part):
    return expert_matrix(key, 4000)


def block_scale(stream_key, extent, cuts, least, high):
    gain, own = 1.0, jax.random.fold_in(stream_key, 6)
    for position, parts in cuts:
        heights = jnp.exp(jax.random.uniform(jax.random.fold_in(own, position), (parts,), jnp.float32, least / len(cuts), high / len(cuts)))
        gain = gain * jnp.repeat(heights, extent[position] // parts).reshape([-1 if axis == position else 1 for axis in range(len(extent))])
    return gain


def deal_out(stream_key, own, number, rows, number_of, top, limit, skew):
    sequence = jax.random.permutation(stream_key, number_of)
    heavy_load, ordinary = shares(number_of, rows * top, limit, skew, True), shares(number_of, rows * top, limit, skew, False)
    places = jnp.arange(number_of)

    def named(tallies, offset_by):
        used = int((tallies > 0).sum())
        fixed = max(1, used // 4)
        shifted = fixed + (places - fixed + offset_by * (used - fixed)) % max(1, number_of - fixed)
        return jnp.zeros((number_of,), jnp.int32).at[sequence[jnp.where(places < fixed, places, shifted)]].set(jnp.asarray(tallies, jnp.int32))

    tallies = jnp.where(number % 4 == 0, named(heavy_load, number // 4), named(ordinary, number - number // 4 - 1))
    mixed = jax.random.permutation(jax.random.fold_in(own, 3), number_of)
    source_of, taker = mixed[0:number_of // 2 * 2:2], mixed[1:number_of // 2 * 2:2]
    slack = jnp.minimum(tallies[source_of] - 1, limit - tallies[taker]) // 2
    slack = jnp.where((source_of == sequence[0]) | (taker == sequence[0]) | (tallies[taker] == 0), 0, jnp.maximum(slack, 0))
    shifted = jax.random.randint(jax.random.fold_in(own, 4), (number_of // 2,), 0, 1 << 20) % (slack + 1)
    tallies = tallies.at[source_of].add(-shifted).at[taker].add(shifted)
    items = jnp.searchsorted(jnp.cumsum(tallies), jnp.arange(rows * top), side="right").astype(jnp.int32)
    grid = items.reshape(top, rows).T
    grid = grid[jax.random.permutation(jax.random.fold_in(own, 1), rows)]
    offset_by = jax.random.randint(jax.random.fold_in(own, 2), (rows, 1), 0, top)
    return jnp.take_along_axis(grid, (jnp.arange(top)[None, :] + offset_by) % top, axis=1)


def shares(number_of, total, most, slope, full):
    weights = [(1 << 20) // math.isqrt(rank ** slope) + 1 for rank in range(1, number_of + 1)]
    largest = most if full else min(most, max(-(-total // number_of), total * weights[0] // sum(weights)))
    least = 1 if total - largest >= number_of - 1 else 0
    given, rest = [largest] + [least] * (number_of - 1), total - largest - least * (number_of - 1)
    while rest > 0:
        free = [i for i in range(1, number_of) if given[i] < largest] or [i for i in range(1, number_of) if given[i] < most]
        whole, remaining = sum([weights[i] for i in free]), rest
        for i in free:
            addition = min(most - given[i], max(1, remaining * weights[i] // whole), rest)
            given[i] = given[i] + addition
            rest = rest - addition
    return np.array(given)


def bell_draw(key, shape, deviation, limit, shards=(), held_as=jnp.bfloat16):
    drawn = deviation * jax.random.normal(key, shape, jnp.float32)
    if shards:
        drawn = drawn * block_scale(key, shape, shards, -0.22, 0.18)
    return jnp.clip(drawn, -limit, limit).astype(held_as)


def setup_inputs(seed: int = 0) -> dict:
    key_list = jax.random.split(jax.random.key(seed), 16)
    queries_a = draw_queries_a(jax.random.fold_in(key_list[15], 71), 0)
    queries_b = draw_queries_b(jax.random.fold_in(key_list[15], 71), 0)
    keys_a = draw_keys_a(jax.random.fold_in(key_list[15], 71), 0)
    keys_b = draw_keys_b(jax.random.fold_in(key_list[15], 71), 0)
    values = bell_draw(key_list[4], (SEQ, KV_HEADS * VDIM), 1.0, 6.0, ((0, 64), (1, 4)))
    lambdas = jnp.clip(0.3 + 0.5 * jax.random.uniform(key_list[5], (HEADS,), jnp.float32) ** block_scale(key_list[5], (HEADS,), ((0, 4),), -0.2, 0.2), 0.3, 0.8)
    head_gain = jnp.clip(1.0 + 0.18 * jax.random.normal(key_list[6], (VDIM,), jnp.float32), 0.1, 1.9)
    w_out = bell_draw(key_list[7], (HEADS * VDIM, D), (HEADS * VDIM) ** -0.5, 0.125, ((0, 4),))
    moe_tokens = draw_moe_tokens(jax.random.fold_in(key_list[15], 71), 0)
    moe_gain = jnp.clip(1.0 + 0.18 * jax.random.normal(key_list[9], (D,), jnp.float32), 0.1, 1.9)
    routes_keys = jax.random.split(jax.random.fold_in(key_list[10], 1), MOE_TOK // TOKB)
    routes_turns = jax.random.permutation(jax.random.fold_in(key_list[10], 3), MOE_TOK // TOKB)
    routes = jax.vmap(lambda own, number: deal_out(jax.random.fold_in(key_list[10], 2), own, number, TOKB, EXPERTS, TOP, CAP, 2))(routes_keys, routes_turns).reshape((MOE_TOK, TOP))
    route_weights = jnp.clip(0.1 + 0.9 * jax.random.uniform(key_list[11], (MOE_TOK, TOP), jnp.float32) ** block_scale(key_list[11], (MOE_TOK, TOP), ((0, 256),), -0.2, 0.2), 0.1, 1.0)
    w_gate = draw_w_gate(jax.random.fold_in(key_list[15], 71), 0)
    w_up = draw_w_up(jax.random.fold_in(key_list[15], 71), 0)
    w_down = bell_draw(key_list[14], (EXPERTS, FF, D), (4 * FF) ** -0.5, 0.0625, ((0, 64), (1, 4)))
    return {"queries_a": queries_a, "queries_b": queries_b, "keys_a": keys_a, "keys_b": keys_b, "values": values, "lambdas": lambdas, "head_gain": head_gain, "w_out": w_out, "moe_tokens": moe_tokens, "moe_gain": moe_gain, "routes": routes, "route_weights": route_weights, "w_gate": w_gate, "w_up": w_up, "w_down": w_down}


eps = 1e-05
alpha_act = 1.702
limit_act = 7.0

def clamped_unit(gate, up):
    capped = jnp.minimum(gate, limit_act)
    linear = jnp.clip(up, -limit_act, limit_act)
    return capped * jax.nn.sigmoid(alpha_act * capped) * (linear + 1.0)

def hidden_rows(inputs, gate_matrix, up_matrix):
    gate = jnp.dot(inputs, gate_matrix, preferred_element_type=jnp.float32)
    up = jnp.dot(inputs, up_matrix, preferred_element_type=jnp.float32)
    return clamped_unit(gate, up).astype(jnp.bfloat16)

def map_weights(queries, keys, value_rows, query_pos, key_pos):
    scores = jnp.dot(queries, keys.T, preferred_element_type=jnp.float32) * HEAD ** (-0.5)
    visible = key_pos[None, :] <= query_pos[:, None]
    scores = jnp.where(visible, scores, -jnp.inf)
    peak = lax.optimization_barrier(jnp.max(scores, axis=1, keepdims=True))
    expo = jnp.where(visible, jnp.exp(scores - peak), 0.0)
    total = lax.optimization_barrier(jnp.sum(expo, axis=1, keepdims=True))
    mixed = jnp.dot(expo.astype(jnp.bfloat16), value_rows, preferred_element_type=jnp.float32)
    return mixed / total

def one_head(head, queries_a, queries_b, keys_a, keys_b, values, lambdas, head_gain):
    kv_head = head // (HEADS // KV_HEADS)
    query_a = lax.dynamic_slice_in_dim(queries_a, (head * HEAD).astype(jnp.int32), HEAD, 1)
    query_b = lax.dynamic_slice_in_dim(queries_b, (head * HEAD).astype(jnp.int32), HEAD, 1)
    key_a = lax.dynamic_slice_in_dim(keys_a, (kv_head * HEAD).astype(jnp.int32), HEAD, 1)
    key_b = lax.dynamic_slice_in_dim(keys_b, (kv_head * HEAD).astype(jnp.int32), HEAD, 1)
    value_head = lax.dynamic_slice_in_dim(values, (kv_head * VDIM).astype(jnp.int32), VDIM, 1)
    key_pos = jnp.arange(SEQ, dtype=jnp.int32)
    strength = lambdas[head]

    def one_block(index):
        start = (index * ATT_DEV).astype(jnp.int32)
        query_pos = start + jnp.arange(ATT_DEV, dtype=jnp.int32)
        first = map_weights(lax.dynamic_slice_in_dim(query_a, start, ATT_DEV, 0), key_a, value_head, query_pos, key_pos)
        second = map_weights(lax.dynamic_slice_in_dim(query_b, start, ATT_DEV, 0), key_b, value_head, query_pos, key_pos)
        diff = first - strength * second
        scaled = diff * lax.rsqrt(lax.optimization_barrier(jnp.mean(diff * diff, axis=-1, keepdims=True)) + eps) * head_gain
        return scaled.astype(jnp.bfloat16)
    return lax.map(one_block, jnp.arange(N_EP, dtype=jnp.int32)).reshape(SEQ, VDIM)

def reference(queries_a, queries_b, keys_a, keys_b, values, lambdas, head_gain, w_out, moe_tokens, moe_gain, routes, route_weights, w_gate, w_up, w_down):
    heads = lax.map(lambda head: one_head(head, queries_a, queries_b, keys_a, keys_b, values, lambdas, head_gain), jnp.arange(HEADS, dtype=jnp.int32))
    heads = heads.transpose(1, 0, 2).reshape(SEQ, N_TP, HEADS // N_TP * VDIM)
    weight_groups = w_out.reshape(N_TP, HEADS // N_TP * VDIM, D)
    head_parts = jnp.einsum('sjc,jcd->jsd', heads.astype(jnp.float32), weight_groups.astype(jnp.float32))
    head_parts = lax.optimization_barrier(head_parts.astype(jnp.bfloat16))
    mixer_out = lax.optimization_barrier(jnp.sum(head_parts.astype(jnp.float32), axis=0)).astype(jnp.bfloat16)
    inputs = moe_tokens.astype(jnp.float32)
    normed = (inputs * lax.rsqrt(lax.optimization_barrier(jnp.mean(inputs * inputs, axis=-1, keepdims=True)) + eps) * moe_gain).astype(jnp.bfloat16)
    blocks = MOE_TOK // TOKB
    chosen = routes.reshape(blocks, TOKB * TOP)
    member = (chosen[:, :, None] == jnp.arange(EXPERTS, dtype=jnp.int32)[None, None, :]).astype(jnp.int32)
    order_in = lax.optimization_barrier(jnp.sum(jnp.cumsum(member, axis=1) * member, axis=2)) - 1
    block_ids = jnp.arange(blocks, dtype=jnp.int32)[:, None]
    slot_ids = ((chosen * blocks + block_ids) * CAP + order_in).astype(jnp.int32)
    token_ids = (block_ids * TOKB + jnp.arange(TOKB * TOP, dtype=jnp.int32)[None, :] // TOP).astype(jnp.int32)
    owner = jnp.full((EXPERTS * blocks * CAP,), MOE_TOK, jnp.int32).at[slot_ids.reshape(-1)].set(token_ids.reshape(-1))
    owner = owner.reshape(EXPERTS, blocks * CAP)

    def one_expert(index):
        slot_owner = owner[index]
        valid = slot_owner < MOE_TOK
        taken = jnp.take(normed, jnp.minimum(slot_owner, MOE_TOK - 1), axis=0)
        taken = jnp.where(valid[:, None], taken, jnp.zeros_like(taken))
        hidden = hidden_rows(taken, w_gate[index], w_up[index])
        unit_parts = jnp.einsum('rjf,jfd->jrd', hidden.reshape(-1, N_TP, FF // N_TP).astype(jnp.float32), w_down[index].reshape(N_TP, FF // N_TP, D).astype(jnp.float32))
        unit_parts = lax.optimization_barrier(unit_parts.astype(jnp.bfloat16))
        return lax.optimization_barrier(jnp.sum(unit_parts.astype(jnp.float32), axis=0)).astype(jnp.bfloat16)
    expert_rows = lax.map(one_expert, jnp.arange(EXPERTS, dtype=jnp.int32))
    picked = jnp.take(expert_rows.reshape(-1, D), slot_ids.reshape(-1), axis=0).reshape(MOE_TOK, TOP, D)
    moe_out = lax.optimization_barrier(jnp.sum(picked.astype(jnp.float32) * route_weights[:, :, None], axis=1)).astype(jnp.bfloat16)
    return (mixer_out, moe_out)
```

```python
import jax
import jax.numpy as jnp
from jax import lax
from jax.experimental import pallas as pl
from jax.experimental.pallas import tpu as pltpu
from jax.sharding import PartitionSpec as P

MESH = pl.DeviceIdType.MESH
BF16 = jnp.bfloat16
F32 = jnp.float32

D = 2048
HEAD = 64
VDIM = 128
N_EP = 64
N_TP = 4
PLANE = 8
ROUNDS = 8
CAP = 6
SLOT = 8
EXPERTS = 64
TOKB = 128
FFL = 512
KBLOCK = 1024

eps = 1e-05
alpha_act = 1.702
limit_act = 7.0
negative = -1e30


def round_offset(t):
    odd = lax.rem(t, 2)
    return odd * lax.div(t + 1, 2) + (1 - odd) * lax.rem(ROUNDS - lax.div(t, 2), ROUNDS)


def wait_for(ref, sem):
    pltpu.make_async_copy(ref, ref, sem).wait()


def moe_kernel(
    tok,
    gain,
    routes,
    rweights,
    wg_hbm,
    wu_hbm,
    wd_hbm,
    out,
    wg,
    wu,
    wd,
    outgoing,
    gathered,
    partial,
    rs1,
    rs2,
    back,
    returned,
    hid,
    w_hi,
    w_lo,
    w_sem,
    disp_send,
    disp_recv,
    ag1_send,
    ag1_recv,
    ag2_send,
    ag2_recv,
    rs1_send,
    rs1_recv,
    rs2_send,
    rs2_recv,
    ret_send,
    ret_recv,
):
    ep = lax.axis_index("ep")
    tp = lax.axis_index("tp")
    z = lax.div(ep, PLANE)
    mine = lax.rem(ep, PLANE)
    left = (ep, lax.rem(tp + N_TP - 1, N_TP))
    right = (ep, lax.rem(tp + 1, N_TP))
    rows = pl.ds(0, CAP)
    half_a, half_b = pl.ds(0, PLANE // 2), pl.ds(PLANE // 2, PLANE // 2)

    def send(src, dst, send_sem, recv_sem, device):
        pltpu.make_async_remote_copy(
            src_ref=src,
            dst_ref=dst,
            send_sem=send_sem,
            recv_sem=recv_sem,
            device_id=device,
            device_id_type=MESH,
        ).start()

    weights = [
        pltpu.make_async_copy(wg_hbm.at[0], wg, w_sem.at[0]),
        pltpu.make_async_copy(wu_hbm.at[0], wu, w_sem.at[1]),
        pltpu.make_async_copy(wd_hbm.at[0], wd, w_sem.at[2]),
    ]
    for copy in weights:
        copy.start()

    slot = lax.broadcasted_iota(jnp.int32, (TOKB, EXPERTS * SLOT), 1)
    expert, place = lax.div(slot, SLOT), lax.rem(slot, SLOT)
    first = routes[:, 0:1] == expert
    second = routes[:, 1:2] == expert
    member = jnp.where(first | second, 1.0, 0.0)
    earlier = lax.broadcasted_iota(jnp.int32, (TOKB, TOKB), 1) < lax.broadcasted_iota(
        jnp.int32, (TOKB, TOKB), 0
    )
    earlier = jnp.where(earlier, 1.0, 0.0).astype(BF16)
    count = jnp.dot(earlier, member.astype(BF16), preferred_element_type=F32)
    chosen = jnp.where(count == place.astype(F32), member, 0.0)
    weight = chosen * jnp.where(first, rweights[:, 0:1], rweights[:, 1:2])
    high = weight.astype(BF16)
    w_hi[...] = high
    w_lo[...] = (weight - high.astype(F32)).astype(BF16)
    inputs = tok[...].astype(F32)
    scale = lax.rsqrt(jnp.mean(inputs * inputs, axis=-1, keepdims=True) + eps)
    normed = (inputs * scale * gain[...]).astype(BF16)
    packed = lax.dot_general(
        chosen.astype(BF16), normed, (((0,), (0,)), ((), ())), preferred_element_type=F32
    )
    outgoing[...] = packed.astype(BF16).reshape(EXPERTS, SLOT, D)
    returned[:, CAP:SLOT, :] = jnp.zeros((EXPERTS, SLOT - CAP, D), BF16)

    def dispatch(t, carry):
        plane = lax.rem(z + round_offset(t), ROUNDS)

        def one(j, carry):
            e = plane * PLANE + j
            src = outgoing.at[e, rows]
            dst = gathered.at[t, 0, mine, rows]

            @pl.when(e != ep)
            def _():
                send(src, dst, disp_send, disp_recv.at[t], (e, tp))

            @pl.when(e == ep)
            def _():
                pltpu.make_async_copy(src, dst, disp_recv.at[t]).start()

            return carry

        return lax.fori_loop(0, PLANE, one, carry)

    lax.fori_loop(0, ROUNDS, dispatch, 0)
    for copy in weights:
        copy.wait()

    def stage_spread(t):
        wait_for(gathered.at[t, 0, :, rows], disp_recv.at[t])
        own = gathered.at[t, 0, :, rows]
        send(own, gathered.at[t, 1, :, rows], ag1_send, ag1_recv.at[t, 0], right)
        send(own, gathered.at[t, 3, :, rows], ag1_send, ag1_recv.at[t, 1], left)

    def stage_forward(t):
        wait_for(gathered.at[t, 1, :, rows], ag1_recv.at[t, 0])
        send(
            gathered.at[t, 1, half_a, rows],
            gathered.at[t, 2, half_a, rows],
            ag2_send,
            ag2_recv.at[t, 0],
            right,
        )
        wait_for(gathered.at[t, 3, :, rows], ag1_recv.at[t, 1])
        send(
            gathered.at[t, 3, half_b, rows],
            gathered.at[t, 2, half_b, rows],
            ag2_send,
            ag2_recv.at[t, 1],
            left,
        )

    def stage_compute(t):
        wait_for(gathered.at[t, 2, half_a, rows], ag2_recv.at[t, 0])
        wait_for(gathered.at[t, 2, half_b, rows], ag2_recv.at[t, 1])
        for n in range(FFL // 256):
            cols = slice(n * 256, (n + 1) * 256)
            x = gathered[t].reshape(N_TP * PLANE * SLOT, D)
            gate = jnp.dot(x, wg[:, cols], preferred_element_type=F32)
            up = jnp.dot(x, wu[:, cols], preferred_element_type=F32)
            capped = jnp.minimum(gate, limit_act)
            linear = jnp.clip(up, -limit_act, limit_act)
            act = capped * jax.nn.sigmoid(alpha_act * capped) * (linear + 1.0)
            hid[:, cols] = act.astype(BF16)

        def down(n, carry):
            cols = pl.ds(pl.multiple_of(n * 512, 512), 512)
            part = jnp.dot(hid[...], wd[:, cols], preferred_element_type=F32)
            partial[t, :, :, :, cols] = part.astype(BF16).reshape(N_TP, PLANE, SLOT, 512)
            return carry

        lax.fori_loop(0, D // 512, down, 0)
        send(
            partial.at[t, 2, half_a, rows],
            rs1.at[t, 0, :, rows],
            rs1_send,
            rs1_recv.at[t, 0],
            right,
        )
        send(
            partial.at[t, 2, half_b, rows], rs1.at[t, 1, :, rows], rs1_send, rs1_recv.at[t, 1], left
        )
        send(
            partial.at[t, 3, half_b, rows],
            rs2.at[t, 0, half_b, rows],
            rs2_send,
            rs2_recv.at[t, 0, 1],
            right,
        )
        send(
            partial.at[t, 1, half_a, rows],
            rs2.at[t, 1, half_a, rows],
            rs2_send,
            rs2_recv.at[t, 1, 0],
            left,
        )

    def stage_add(t):
        wait_for(rs1.at[t, 0, :, rows], rs1_recv.at[t, 0])
        summed = partial[t, 3, half_a].astype(F32) + rs1[t, 0].astype(F32)
        partial[t, 3, half_a] = summed.astype(BF16)
        send(
            partial.at[t, 3, half_a, rows],
            rs2.at[t, 0, half_a, rows],
            rs2_send,
            rs2_recv.at[t, 0, 0],
            right,
        )
        wait_for(rs1.at[t, 1, :, rows], rs1_recv.at[t, 1])
        summed = partial[t, 1, half_b].astype(F32) + rs1[t, 1].astype(F32)
        partial[t, 1, half_b] = summed.astype(BF16)
        send(
            partial.at[t, 1, half_b, rows],
            rs2.at[t, 1, half_b, rows],
            rs2_send,
            rs2_recv.at[t, 1, 1],
            left,
        )

    def stage_return(t):
        for side in range(2):
            wait_for(rs2.at[t, side, half_a, rows], rs2_recv.at[t, side, 0])
            wait_for(rs2.at[t, side, half_b, rows], rs2_recv.at[t, side, 1])
        summed = partial[t, 0].astype(F32) + rs2[t, 0].astype(F32) + rs2[t, 1].astype(F32)
        back[t] = summed.astype(BF16)
        plane = lax.rem(z + ROUNDS - round_offset(t), ROUNDS)

        def one(j, carry):
            e = plane * PLANE + j
            src = back.at[t, j, rows]
            dst = returned.at[ep, rows]

            @pl.when(e != ep)
            def _():
                send(src, dst, ret_send, ret_recv, (e, tp))

            @pl.when(e == ep)
            def _():
                pltpu.make_async_copy(src, dst, ret_recv).start()

            return carry

        lax.fori_loop(0, PLANE, one, 0)

    stages = (stage_spread, stage_forward, stage_compute, stage_add, stage_return)

    def tick(i, carry):
        for lag in range(len(stages)):

            @pl.when((i >= lag) & (i - lag < ROUNDS))
            def _(lag=lag):
                stages[lag](i - lag)

        return carry

    lax.fori_loop(0, ROUNDS + len(stages) - 1, tick, 0)

    wait_for(returned.at[:, rows], ret_recv)

    def combine(n, carry):
        cols = pl.ds(pl.multiple_of(n * 512, 512), 512)
        table = returned[:, :, cols].reshape(EXPERTS * SLOT, 512)
        total = jnp.dot(w_hi[...], table, preferred_element_type=F32)
        total = total + jnp.dot(w_lo[...], table, preferred_element_type=F32)
        out[:, cols] = total.astype(BF16)
        return carry

    lax.fori_loop(0, D // 512, combine, 0)

    some = pl.ds(0, N_EP - 1)
    wait_for(outgoing.at[some, rows], disp_send)
    wait_for(returned.at[some, rows], ret_send)
    wait_for(gathered.at[:, 0:2, :, rows], ag1_send)
    wait_for(back.at[:, :, rows], ag2_send)
    wait_for(back.at[:, :, rows], rs1_send)
    wait_for(gathered.at[:, 0:2, :, rows], rs2_send)


def moe(moe_tokens, moe_gain, routes, route_weights, w_gate, w_up, w_down):
    dma = pltpu.SemaphoreType.DMA
    vmem = pl.BlockSpec(memory_space=pltpu.VMEM)
    hbm = pl.BlockSpec(memory_space=pl.ANY)
    return pl.pallas_call(
        moe_kernel,
        out_shape=jax.ShapeDtypeStruct((TOKB, D), BF16),
        in_specs=[vmem] * 4 + [hbm] * 3,
        out_specs=vmem,
        scratch_shapes=[
            pltpu.VMEM((D, FFL), BF16),
            pltpu.VMEM((D, FFL), BF16),
            pltpu.VMEM((FFL, D), BF16),
            pltpu.VMEM((EXPERTS, SLOT, D), BF16),
            pltpu.VMEM((ROUNDS, N_TP, PLANE, SLOT, D), BF16),
            pltpu.VMEM((ROUNDS, N_TP, PLANE, SLOT, D), BF16),
            pltpu.VMEM((ROUNDS, 2, PLANE // 2, SLOT, D), BF16),
            pltpu.VMEM((ROUNDS, 2, PLANE, SLOT, D), BF16),
            pltpu.VMEM((ROUNDS, PLANE, SLOT, D), BF16),
            pltpu.VMEM((EXPERTS, SLOT, D), BF16),
            pltpu.VMEM((N_TP * PLANE * SLOT, FFL), BF16),
            pltpu.VMEM((TOKB, EXPERTS * SLOT), BF16),
            pltpu.VMEM((TOKB, EXPERTS * SLOT), BF16),
            dma((3,)),
            dma,
            dma((ROUNDS,)),
            dma,
            dma((ROUNDS, 2)),
            dma,
            dma((ROUNDS, 2)),
            dma,
            dma((ROUNDS, 2)),
            dma,
            dma((ROUNDS, 2, 2)),
            dma,
            dma,
        ],
        compiler_params=pltpu.CompilerParams(
            has_side_effects=True, vmem_limit_bytes=58 * 1024 * 1024
        ),
        cost_estimate=pl.CostEstimate(
            flops=100_000_000_000, bytes_accessed=8_000_000, transcendentals=0
        ),
        name="experts",
    )(moe_tokens, moe_gain.reshape(1, D), routes, route_weights, w_gate, w_up, w_down)


def attention_kernel(qa, qb, kv, lambdas, gain, w_out, out, qp, peak, accum, heads):
    ep = lax.axis_index("ep")
    block = pl.program_id(0)
    group = 2 * TOKB

    @pl.when(block == 0)
    def _():
        peak[...] = jnp.full_like(peak, negative)
        accum[...] = jnp.zeros_like(accum)
        lane = lax.broadcasted_iota(jnp.int32, (TOKB, 128), 1)
        zero = jnp.zeros((TOKB, 128), BF16)
        for which, source in enumerate((qa, qb)):
            for g in range(2):
                pair = source[:, g * 128 : (g + 1) * 128].astype(F32) * HEAD**-0.5
                for j in range(2):
                    turned = pair if g == j else pltpu.roll(pair, 64, 1)
                    part = jnp.where((lane >= 64) == (g == 1), turned, 0.0).astype(BF16)
                    base = (which * 2 + g) * group + j * TOKB
                    qp[base : base + TOKB, which * 128 : (which + 1) * 128] = part
                    other = 1 - which
                    qp[base : base + TOKB, other * 128 : (other + 1) * 128] = zero

    def visit(masked):
        if masked:
            row = lax.broadcasted_iota(jnp.int32, (group, KBLOCK), 0)
            key = lax.broadcasted_iota(jnp.int32, (group, KBLOCK), 1) + block * KBLOCK
            visible = key <= ep * TOKB + lax.rem(row, TOKB)
        for which in range(2):
            for g in range(2):
                at = slice((which * 2 + g) * group, (which * 2 + g + 1) * group)
                scores = lax.dot_general(
                    qp[at, :],
                    kv[:, 0:256],
                    (((1,), (1,)), ((), ())),
                    preferred_element_type=F32,
                )
                if masked:
                    scores = jnp.where(visible, scores, negative)
                old = peak[at, :]
                new = jnp.maximum(old, jnp.max(scores, axis=1, keepdims=True))
                expo = jnp.exp(scores - new[:, 0:1])
                values = kv[:, 256 + g * VDIM : 256 + (g + 1) * VDIM]
                values = jnp.concatenate([values, jnp.ones_like(values)], axis=1)
                mixed = jnp.dot(expo.astype(BF16), values, preferred_element_type=F32)
                fade = jnp.exp(old - new)
                accum[at, 0:VDIM] = accum[at, 0:VDIM] * fade + mixed[:, 0:VDIM]
                accum[at, VDIM:] = accum[at, VDIM:] * fade + mixed[:, VDIM:]
                peak[at, :] = new

    begin, start = block * KBLOCK, ep * TOKB

    @pl.when(begin + KBLOCK - 1 <= start)
    def _():
        visit(False)

    @pl.when((begin + KBLOCK - 1 > start) & (begin <= start + TOKB - 1))
    def _():
        visit(True)

    @pl.when(block == pl.num_programs(0) - 1)
    def _():
        for g in range(2):
            for j in range(2):
                h = g * 2 + j
                a = slice(g * group + j * TOKB, g * group + (j + 1) * TOKB)
                b = slice((2 + g) * group + j * TOKB, (2 + g) * group + (j + 1) * TOKB)
                diff = accum[a, 0:VDIM] / accum[a, VDIM:] - lambdas[h] * (
                    accum[b, 0:VDIM] / accum[b, VDIM:]
                )
                scale = lax.rsqrt(jnp.mean(diff * diff, axis=-1, keepdims=True) + eps)
                heads[:, h * VDIM : (h + 1) * VDIM] = (diff * scale * gain[...]).astype(BF16)
        out[...] = jnp.dot(heads[...], w_out[...], preferred_element_type=F32).astype(BF16)


def attention(queries_a, queries_b, keys_a, keys_b, values, lambdas, head_gain, w_out):
    own = jnp.concatenate([keys_a, keys_b, values], axis=1)
    kv = lax.all_gather(own, "ep", axis=0, tiled=True)
    blocks = kv.shape[0] // KBLOCK
    whole = lambda *shape: pl.BlockSpec(shape, lambda i: (0,) * len(shape))
    parts = pl.pallas_call(
        attention_kernel,
        grid=(blocks,),
        out_shape=jax.ShapeDtypeStruct((TOKB, D), BF16),
        in_specs=[
            whole(TOKB, 256),
            whole(TOKB, 256),
            pl.BlockSpec((KBLOCK, 512), lambda i: (i, 0)),
            pl.BlockSpec(memory_space=pltpu.SMEM),
            whole(1, VDIM),
            whole(512, D),
        ],
        out_specs=whole(TOKB, D),
        scratch_shapes=[
            pltpu.VMEM((1024, 256), BF16),
            pltpu.VMEM((1024, 128), F32),
            pltpu.VMEM((1024, 256), F32),
            pltpu.VMEM((TOKB, 512), BF16),
        ],
        compiler_params=pltpu.CompilerParams(
            dimension_semantics=("arbitrary",), vmem_limit_bytes=40 * 1024 * 1024
        ),
        cost_estimate=pl.CostEstimate(
            flops=6_000_000_000, bytes_accessed=11_000_000, transcendentals=8_400_000
        ),
        name="attention",
    )(queries_a, queries_b, kv, lambdas, head_gain.reshape(1, VDIM), w_out)
    pieces = lax.all_to_all(
        parts.reshape(N_TP, TOKB // N_TP, D), "tp", split_axis=0, concat_axis=0, tiled=True
    )
    return jnp.sum(pieces.astype(F32), axis=0).astype(BF16)


def body(
    queries_a,
    queries_b,
    keys_a,
    keys_b,
    values,
    lambdas,
    head_gain,
    w_out,
    moe_tokens,
    moe_gain,
    routes,
    route_weights,
    w_gate,
    w_up,
    w_down,
):
    moe_out = moe(moe_tokens, moe_gain, routes, route_weights, w_gate, w_up, w_down)
    queries_a, moe_out = lax.optimization_barrier((queries_a, moe_out))
    mixer_out = attention(queries_a, queries_b, keys_a, keys_b, values, lambdas, head_gain, w_out)
    return (mixer_out, moe_out)


def solution(mesh):
    return jax.shard_map(
        body,
        mesh=mesh,
        in_specs=(
            P("ep", "tp"),
            P("ep", "tp"),
            P("ep", "tp"),
            P("ep", "tp"),
            P("ep", "tp"),
            P("tp"),
            P(),
            P("tp", None),
            P(("ep", "tp"), None),
            P(),
            P(("ep", "tp"), None),
            P(("ep", "tp"), None),
            P("ep", None, "tp"),
            P("ep", None, "tp"),
            P("ep", "tp", None),
        ),
        out_specs=(P(("ep", "tp"), None), P(("ep", "tp"), None)),
        check_vma=False,
    )
```

```python
import jax
import jax.numpy as jnp
from jax import lax
from jax.experimental import pallas as pl
from jax.experimental.pallas import tpu as pltpu
from jax.sharding import PartitionSpec as P

MESH = pl.DeviceIdType.MESH
BF16 = jnp.bfloat16
F32 = jnp.float32

D = 2048
HEAD = 64
VDIM = 128
N_EP = 64
N_TP = 4
PLANE = 8
ROUNDS = 8
CAP = 6
SLOT = 8
EXPERTS = 64
TOKB = 128
FFL = 512
KBLOCK = 1024
KV_LAG = 3
KV_PER_TICK = 2

eps = 1e-05
alpha_act = 1.702
limit_act = 7.0
negative = -1e30


def round_offset(t):
    odd = lax.rem(t, 2)
    return odd * lax.div(t + 1, 2) + (1 - odd) * lax.rem(ROUNDS - lax.div(t, 2), ROUNDS)


def wait_for(ref, sem):
    pltpu.make_async_copy(ref, ref, sem).wait()


def kernel(
    tok,
    gain,
    routes,
    rweights,
    qa,
    qb,
    lambdas,
    head_gain,
    ka_hbm,
    kb_hbm,
    v_hbm,
    wo_hbm,
    wg_hbm,
    wu_hbm,
    wd_hbm,
    out,
    mixer,
    wg,
    wu,
    wd,
    outgoing,
    gathered,
    partial,
    rs1,
    rs2,
    back,
    returned,
    hid,
    w_hi,
    w_lo,
    kv,
    wo,
    qp,
    peak,
    accum,
    heads,
    shares,
    arrived,
    w_sem,
    kv_sem,
    disp_send,
    disp_recv,
    ag1_send,
    ag1_recv,
    ag2_send,
    ag2_recv,
    rs1_send,
    rs1_recv,
    rs2_send,
    rs2_recv,
    ret_send,
    ret_recv,
    kvz_send,
    kvz_recv,
    ky1_send,
    ky1_recv,
    ky2_send,
    ky2_recv,
    kp_send,
    kp_recv,
    mx_send,
    mx_recv,
):
    ep = lax.axis_index("ep")
    tp = lax.axis_index("tp")
    z = lax.div(ep, PLANE)
    mine = lax.rem(ep, PLANE)
    y, core = lax.div(mine, 2), lax.rem(mine, 2)
    left = (ep, lax.rem(tp + N_TP - 1, N_TP))
    right = (ep, lax.rem(tp + 1, N_TP))
    y_down, y_up, y_far = lax.rem(y + 3, 4), lax.rem(y + 1, 4), lax.rem(y + 2, 4)
    b_down, b_up, b_far = y_down * 2 + core, y_up * 2 + core, y_far * 2 + core
    up, down = (z * PLANE + b_up, tp), (z * PLANE + b_down, tp)
    peer = (z * PLANE + y * 2 + 1 - core, tp)
    rows = pl.ds(0, CAP)
    half_a, half_b = pl.ds(0, PLANE // 2), pl.ds(PLANE // 2, PLANE // 2)

    def send(src, dst, send_sem, recv_sem, device):
        pltpu.make_async_remote_copy(
            src_ref=src,
            dst_ref=dst,
            send_sem=send_sem,
            recv_sem=recv_sem,
            device_id=device,
            device_id_type=MESH,
        ).start()

    own_kv = [
        pltpu.make_async_copy(ka_hbm, kv.at[z, mine, :, 0:128], kv_sem.at[0]),
        pltpu.make_async_copy(kb_hbm, kv.at[z, mine, :, 128:256], kv_sem.at[1]),
        pltpu.make_async_copy(v_hbm, kv.at[z, mine, :, 256:512], kv_sem.at[2]),
    ]
    weights = [
        pltpu.make_async_copy(wg_hbm.at[0], wg, w_sem.at[0]),
        pltpu.make_async_copy(wu_hbm.at[0], wu, w_sem.at[1]),
        pltpu.make_async_copy(wd_hbm.at[0], wd, w_sem.at[2]),
        pltpu.make_async_copy(wo_hbm, wo, w_sem.at[3]),
    ]
    for copy in own_kv + weights:
        copy.start()

    slot = lax.broadcasted_iota(jnp.int32, (EXPERTS * SLOT, TOKB), 0)
    expert, place = lax.div(slot, SLOT), lax.rem(slot, SLOT)
    first = routes[0:1, :] == expert
    second = routes[1:2, :] == expert
    member = jnp.where(first | second, 1.0, 0.0)
    earlier = lax.broadcasted_iota(jnp.int32, (TOKB, TOKB), 0) < lax.broadcasted_iota(
        jnp.int32, (TOKB, TOKB), 1
    )
    earlier = jnp.where(earlier, 1.0, 0.0).astype(BF16)
    count = jnp.dot(member.astype(BF16), earlier, preferred_element_type=F32)
    chosen = jnp.where(count == place.astype(F32), member, 0.0)
    inputs = tok[...].astype(F32)
    scale = lax.rsqrt(jnp.mean(inputs * inputs, axis=-1, keepdims=True) + eps)
    normed = (inputs * scale * gain[...]).astype(BF16)
    packed = jnp.dot(chosen.astype(BF16), normed, preferred_element_type=F32)
    outgoing[...] = packed.astype(BF16).reshape(EXPERTS, SLOT, D)

    def dispatch(t, carry):
        plane = lax.rem(z + round_offset(t), ROUNDS)

        def one(j, carry):
            e = plane * PLANE + j
            src = outgoing.at[e, rows]
            dst = gathered.at[t, 0, mine, rows]

            @pl.when(e != ep)
            def _():
                send(src, dst, disp_send, disp_recv.at[t], (e, tp))

            @pl.when(e == ep)
            def _():
                pltpu.make_async_copy(src, dst, disp_recv.at[t]).start()

            return carry

        return lax.fori_loop(0, PLANE, one, carry)

    lax.fori_loop(0, ROUNDS, dispatch, 0)

    for copy in own_kv:
        copy.wait()

    def kv_along_z(k, carry):
        @pl.when(z + k < ROUNDS)
        def _():
            block = kv.at[z, mine]
            send(block, block, kvz_send.at[k], kvz_recv.at[k], ((z + k) * PLANE + mine, tp))

        return carry

    lax.fori_loop(1, ROUNDS, kv_along_z, 0)

    weight = jnp.transpose(chosen * jnp.where(first, rweights[0:1, :], rweights[1:2, :]))
    high = weight.astype(BF16)
    w_hi[...] = high
    w_lo[...] = (weight - high.astype(F32)).astype(BF16)
    returned[:, CAP:SLOT, :] = jnp.zeros((EXPERTS, SLOT - CAP, D), BF16)

    group = 2 * TOKB
    peak[...] = jnp.full_like(peak, negative)
    accum[...] = jnp.zeros_like(accum)
    lane = lax.broadcasted_iota(jnp.int32, (TOKB, 128), 1)
    for which, source in enumerate((qa, qb)):
        for g in range(2):
            pair = source[:, g * 128 : (g + 1) * 128].astype(F32) * HEAD**-0.5
            for j in range(2):
                turned = pair if g == j else pltpu.roll(pair, 64, 1)
                part = jnp.where((lane >= 64) == (g == 1), turned, 0.0).astype(BF16)
                base = (which * 2 + g) * group + j * TOKB
                qp[base : base + TOKB, which * 128 : (which + 1) * 128] = part
                other = 1 - which
                qp[base : base + TOKB, other * 128 : (other + 1) * 128] = jnp.zeros_like(part)

    for copy in weights:
        copy.wait()

    def stage_spread(t):
        wait_for(gathered.at[t, 0, :, rows], disp_recv.at[t])
        own = gathered.at[t, 0, :, rows]
        send(own, gathered.at[t, 1, :, rows], ag1_send, ag1_recv.at[t, 0], right)
        send(own, gathered.at[t, 3, :, rows], ag1_send, ag1_recv.at[t, 1], left)

    def stage_forward(t):
        wait_for(gathered.at[t, 1, :, rows], ag1_recv.at[t, 0])
        send(
            gathered.at[t, 1, half_a, rows],
            gathered.at[t, 2, half_a, rows],
            ag2_send,
            ag2_recv.at[t, 0],
            right,
        )
        wait_for(gathered.at[t, 3, :, rows], ag1_recv.at[t, 1])
        send(
            gathered.at[t, 3, half_b, rows],
            gathered.at[t, 2, half_b, rows],
            ag2_send,
            ag2_recv.at[t, 1],
            left,
        )

    def stage_compute(t):
        wait_for(gathered.at[t, 2, half_a, rows], ag2_recv.at[t, 0])
        wait_for(gathered.at[t, 2, half_b, rows], ag2_recv.at[t, 1])
        for n in range(FFL // 256):
            cols = slice(n * 256, (n + 1) * 256)
            x = gathered[t].reshape(N_TP * PLANE * SLOT, D)
            gate = jnp.dot(x, wg[:, cols], preferred_element_type=F32)
            up = jnp.dot(x, wu[:, cols], preferred_element_type=F32)
            capped = jnp.minimum(gate, limit_act)
            linear = jnp.clip(up, -limit_act, limit_act)
            act = capped * jax.nn.sigmoid(alpha_act * capped) * (linear + 1.0)
            hid[:, cols] = act.astype(BF16)

        def down_cols(n, carry):
            cols = pl.ds(pl.multiple_of(n * 512, 512), 512)
            part = jnp.dot(hid[...], wd[:, cols], preferred_element_type=F32)
            partial[t, :, :, :, cols] = part.astype(BF16).reshape(N_TP, PLANE, SLOT, 512)
            return carry

        lax.fori_loop(0, D // 512, down_cols, 0)
        send(
            partial.at[t, 2, half_a, rows],
            rs1.at[t, 0, :, rows],
            rs1_send,
            rs1_recv.at[t, 0],
            right,
        )
        send(
            partial.at[t, 2, half_b, rows], rs1.at[t, 1, :, rows], rs1_send, rs1_recv.at[t, 1], left
        )
        send(
            partial.at[t, 3, half_b, rows],
            rs2.at[t, 0, half_b, rows],
            rs2_send,
            rs2_recv.at[t, 0, 1],
            right,
        )
        send(
            partial.at[t, 1, half_a, rows],
            rs2.at[t, 1, half_a, rows],
            rs2_send,
            rs2_recv.at[t, 1, 0],
            left,
        )

    def stage_add(t):
        wait_for(rs1.at[t, 0, :, rows], rs1_recv.at[t, 0])
        summed = partial[t, 3, half_a].astype(F32) + rs1[t, 0].astype(F32)
        partial[t, 3, half_a] = summed.astype(BF16)
        send(
            partial.at[t, 3, half_a, rows],
            rs2.at[t, 0, half_a, rows],
            rs2_send,
            rs2_recv.at[t, 0, 0],
            right,
        )
        wait_for(rs1.at[t, 1, :, rows], rs1_recv.at[t, 1])
        summed = partial[t, 1, half_b].astype(F32) + rs1[t, 1].astype(F32)
        partial[t, 1, half_b] = summed.astype(BF16)
        send(
            partial.at[t, 1, half_b, rows],
            rs2.at[t, 1, half_b, rows],
            rs2_send,
            rs2_recv.at[t, 1, 1],
            left,
        )

    def stage_return(t):
        for side in range(2):
            wait_for(rs2.at[t, side, half_a, rows], rs2_recv.at[t, side, 0])
            wait_for(rs2.at[t, side, half_b, rows], rs2_recv.at[t, side, 1])
        summed = partial[t, 0].astype(F32) + rs2[t, 0].astype(F32) + rs2[t, 1].astype(F32)
        back[t] = summed.astype(BF16)
        plane = lax.rem(z + ROUNDS - round_offset(t), ROUNDS)

        def one(j, carry):
            e = plane * PLANE + j
            src = back.at[t, j, rows]
            dst = returned.at[ep, rows]

            @pl.when(e != ep)
            def _():
                send(src, dst, ret_send, ret_recv, (e, tp))

            @pl.when(e == ep)
            def _():
                pltpu.make_async_copy(src, dst, ret_recv).start()

            return carry

        lax.fori_loop(0, PLANE, one, 0)

    def kv_spread(k):
        @pl.when(k > 0)
        def _():
            wait_for(kv.at[0, 0], kvz_recv.at[k])

        block = kv.at[z - k, mine]
        send(block, block, ky1_send.at[k], ky1_recv.at[k, 0], up)
        send(block, block, ky1_send.at[k], ky1_recv.at[k, 1], down)
        send(block, block, kp_send.at[k], kp_recv.at[k], peer)

    def kv_forward(k):
        near, far = pl.ds(0, TOKB // 2), pl.ds(TOKB // 2, TOKB // 2)
        block, part = kv.at[z - k, b_down], kv.at[z - k, b_down, near]
        wait_for(block, ky1_recv.at[k, 0])
        send(part, part, ky2_send.at[k], ky2_recv.at[k, 0], up)
        send(block, block, kp_send.at[k], kp_recv.at[k], peer)
        block, part = kv.at[z - k, b_up], kv.at[z - k, b_up, far]
        wait_for(block, ky1_recv.at[k, 1])
        send(part, part, ky2_send.at[k], ky2_recv.at[k, 1], down)
        send(block, block, kp_send.at[k], kp_recv.at[k], peer)

    def kv_share(k):
        block = kv.at[z - k, b_far]
        wait_for(kv.at[z - k, b_far, pl.ds(0, TOKB // 2)], ky2_recv.at[k, 0])
        wait_for(kv.at[z - k, b_far, pl.ds(TOKB // 2, TOKB // 2)], ky2_recv.at[k, 1])
        send(block, block, kp_send.at[k], kp_recv.at[k], peer)

    def visit(plane, masked):
        if masked:
            row = lax.broadcasted_iota(jnp.int32, (group, KBLOCK), 0)
            key = lax.broadcasted_iota(jnp.int32, (group, KBLOCK), 1)
            visible = key <= mine * TOKB + lax.rem(row, TOKB)
        for which in range(2):
            for g in range(2):
                at = slice((which * 2 + g) * group, (which * 2 + g + 1) * group)
                scores = lax.dot_general(
                    qp[at, :],
                    kv[plane, :, :, 0:256].reshape(KBLOCK, 256),
                    (((1,), (1,)), ((), ())),
                    preferred_element_type=F32,
                )
                if masked:
                    scores = jnp.where(visible, scores, negative)
                old = peak[at, :]
                new = jnp.maximum(old, jnp.max(scores, axis=1, keepdims=True))
                expo = jnp.exp(scores - new[:, 0:1])
                values = kv[plane, :, :, 256 + g * VDIM : 256 + (g + 1) * VDIM]
                values = values.reshape(KBLOCK, VDIM)
                values = jnp.concatenate([values, jnp.ones_like(values)], axis=1)
                mixed = jnp.dot(expo.astype(BF16), values, preferred_element_type=F32)
                fade = jnp.exp(old - new)
                accum[at, 0:VDIM] = accum[at, 0:VDIM] * fade + mixed[:, 0:VDIM]
                accum[at, VDIM:] = accum[at, VDIM:] * fade + mixed[:, VDIM:]
                peak[at, :] = new

    def kv_visit(k):
        wait_for(kv.at[0, half_a], kp_recv.at[k])

        @pl.when(k == 0)
        def _():
            visit(z, True)

        @pl.when(k > 0)
        def _():
            visit(z - k, False)

    def project():
        for g in range(2):
            for j in range(2):
                h = g * 2 + j
                a = slice(g * group + j * TOKB, g * group + (j + 1) * TOKB)
                b = slice((2 + g) * group + j * TOKB, (2 + g) * group + (j + 1) * TOKB)
                diff = accum[a, 0:VDIM] / accum[a, VDIM:] - lambdas[h] * (
                    accum[b, 0:VDIM] / accum[b, VDIM:]
                )
                scale = lax.rsqrt(jnp.mean(diff * diff, axis=-1, keepdims=True) + eps)
                heads[:, h * VDIM : (h + 1) * VDIM] = (diff * scale * head_gain[...]).astype(BF16)

        def columns(n, carry):
            cols = pl.ds(pl.multiple_of(n * 512, 512), 512)
            part = jnp.dot(heads[...], wo[:, cols], preferred_element_type=F32)
            shares[:, :, cols] = part.astype(BF16).reshape(N_TP, TOKB // N_TP, 512)
            return carry

        lax.fori_loop(0, D // 512, columns, 0)
        for k in range(1, N_TP):
            to = lax.rem(tp + k, N_TP)
            send(shares.at[to], arrived.at[k - 1], mx_send.at[k - 1], mx_recv.at[k - 1], (ep, to))

    stages = (stage_spread, stage_forward, stage_compute, stage_add, stage_return)
    kv_stages = (kv_spread, kv_forward, kv_share, kv_visit)
    kv_ticks = ROUNDS // KV_PER_TICK

    def tick(i, carry):
        for lag in range(len(stages)):

            @pl.when((i >= lag) & (i - lag < ROUNDS))
            def _(lag=lag):
                stages[lag](i - lag)

        for lag in range(len(kv_stages)):
            m = i - KV_LAG - lag

            @pl.when((m >= 0) & (m < kv_ticks))
            def _(lag=lag, m=m):
                def one(n, carry):
                    k = m * KV_PER_TICK + n

                    @pl.when(k <= z)
                    def _():
                        kv_stages[lag](k)

                    return carry

                lax.fori_loop(0, KV_PER_TICK, one, 0)

        @pl.when(i == KV_LAG + kv_ticks + len(kv_stages) - 1)
        def _():
            project()

        return carry

    lax.fori_loop(0, ROUNDS + len(stages) - 1, tick, 0)

    total = shares[tp].astype(F32)
    for k in range(N_TP - 1):
        wait_for(arrived.at[k], mx_recv.at[k])
        total = total + arrived[k].astype(F32)
    mixer[...] = total.astype(BF16)

    wait_for(returned.at[:, rows], ret_recv)

    def combine(n, carry):
        cols = pl.ds(pl.multiple_of(n * 512, 512), 512)
        table = returned[:, :, cols].reshape(EXPERTS * SLOT, 512)
        total = jnp.dot(w_hi[...], table, preferred_element_type=F32)
        total = total + jnp.dot(w_lo[...], table, preferred_element_type=F32)
        out[:, cols] = total.astype(BF16)
        return carry

    lax.fori_loop(0, D // 512, combine, 0)

    some = pl.ds(0, N_EP - 1)
    wait_for(outgoing.at[some, rows], disp_send)
    wait_for(returned.at[some, rows], ret_send)
    wait_for(gathered.at[:, 0:2, :, rows], ag1_send)
    wait_for(back.at[:, :, rows], ag2_send)
    wait_for(back.at[:, :, rows], rs1_send)
    wait_for(gathered.at[:, 0:2, :, rows], rs2_send)
    for k in range(N_TP - 1):
        wait_for(arrived.at[k], mx_send.at[k])

    def kv_sent(k, carry):
        @pl.when((k > 0) & (z + k < ROUNDS))
        def _():
            wait_for(kv.at[0, 0], kvz_send.at[k])

        @pl.when(k <= z)
        def _():
            wait_for(kv.at[0, 0:2], ky1_send.at[k])
            wait_for(kv.at[0, 0], ky2_send.at[k])
            wait_for(kv.at[0, half_a], kp_send.at[k])

        return carry

    lax.fori_loop(0, ROUNDS, kv_sent, 0)


def body(
    queries_a,
    queries_b,
    keys_a,
    keys_b,
    values,
    lambdas,
    head_gain,
    w_out,
    moe_tokens,
    moe_gain,
    routes,
    route_weights,
    w_gate,
    w_up,
    w_down,
):
    dma = pltpu.SemaphoreType.DMA
    vmem = pl.BlockSpec(memory_space=pltpu.VMEM)
    hbm = pl.BlockSpec(memory_space=pl.ANY)
    moe_out, mixer_out = pl.pallas_call(
        kernel,
        out_shape=(
            jax.ShapeDtypeStruct((TOKB, D), BF16),
            jax.ShapeDtypeStruct((TOKB // N_TP, D), BF16),
        ),
        in_specs=[vmem] * 6 + [pl.BlockSpec(memory_space=pltpu.SMEM), vmem] + [hbm] * 7,
        out_specs=(vmem, vmem),
        scratch_shapes=[
            pltpu.VMEM((D, FFL), BF16),
            pltpu.VMEM((D, FFL), BF16),
            pltpu.VMEM((FFL, D), BF16),
            pltpu.VMEM((EXPERTS, SLOT, D), BF16),
            pltpu.VMEM((ROUNDS, N_TP, PLANE, SLOT, D), BF16),
            pltpu.VMEM((ROUNDS, N_TP, PLANE, SLOT, D), BF16),
            pltpu.VMEM((ROUNDS, 2, PLANE // 2, SLOT, D), BF16),
            pltpu.VMEM((ROUNDS, 2, PLANE, SLOT, D), BF16),
            pltpu.VMEM((ROUNDS, PLANE, SLOT, D), BF16),
            pltpu.VMEM((EXPERTS, SLOT, D), BF16),
            pltpu.VMEM((N_TP * PLANE * SLOT, FFL), BF16),
            pltpu.VMEM((TOKB, EXPERTS * SLOT), BF16),
            pltpu.VMEM((TOKB, EXPERTS * SLOT), BF16),
            pltpu.VMEM((ROUNDS, PLANE, TOKB, 512), BF16),
            pltpu.VMEM((512, D), BF16),
            pltpu.VMEM((8 * TOKB, 256), BF16),
            pltpu.VMEM((8 * TOKB, 128), F32),
            pltpu.VMEM((8 * TOKB, 256), F32),
            pltpu.VMEM((TOKB, 512), BF16),
            pltpu.VMEM((N_TP, TOKB // N_TP, D), BF16),
            pltpu.VMEM((N_TP - 1, TOKB // N_TP, D), BF16),
            dma((4,)),
            dma((3,)),
            dma,
            dma((ROUNDS,)),
            dma,
            dma((ROUNDS, 2)),
            dma,
            dma((ROUNDS, 2)),
            dma,
            dma((ROUNDS, 2)),
            dma,
            dma((ROUNDS, 2, 2)),
            dma,
            dma,
            dma((ROUNDS,)),
            dma((ROUNDS,)),
            dma((ROUNDS,)),
            dma((ROUNDS, 2)),
            dma((ROUNDS,)),
            dma((ROUNDS, 2)),
            dma((ROUNDS,)),
            dma((ROUNDS,)),
            dma((N_TP - 1,)),
            dma((N_TP - 1,)),
        ],
        compiler_params=pltpu.CompilerParams(
            has_side_effects=True, vmem_limit_bytes=60 * 1024 * 1024
        ),
        name="layer",
    )(
        moe_tokens,
        moe_gain.reshape(1, D),
        routes.T,
        route_weights.T,
        queries_a,
        queries_b,
        lambdas,
        head_gain.reshape(1, VDIM),
        keys_a,
        keys_b,
        values,
        w_out,
        w_gate,
        w_up,
        w_down,
    )
    return (mixer_out, moe_out)


def solution(mesh):
    return jax.shard_map(
        body,
        mesh=mesh,
        in_specs=(
            P("ep", "tp"),
            P("ep", "tp"),
            P("ep", "tp"),
            P("ep", "tp"),
            P("ep", "tp"),
            P("tp"),
            P(),
            P("tp", None),
            P(("ep", "tp"), None),
            P(),
            P(("ep", "tp"), None),
            P(("ep", "tp"), None),
            P("ep", None, "tp"),
            P("ep", None, "tp"),
            P("ep", "tp", None),
        ),
        out_specs=(P(("ep", "tp"), None), P(("ep", "tp"), None)),
        check_vma=False,
    )
```

```python
import jax
import jax.numpy as jnp
from jax import lax
from jax.experimental import pallas as pl
from jax.experimental.pallas import tpu as pltpu
from jax.sharding import PartitionSpec as P

MESH = pl.DeviceIdType.MESH
BF16 = jnp.bfloat16
F32 = jnp.float32

D = 2048
HEAD = 64
VDIM = 128
N_EP = 64
N_TP = 4
PLANE = 8
Z = 8
SPLIT = 2
ROUNDS = Z * SPLIT
SOURCES = PLANE // SPLIT
CAP = 6
SLOT = 8
EXPERTS = 64
TOKB = 128
FFL = 512
KBLOCK = 1024
KV_LAG = 6

eps = 1e-05
alpha_act = 1.702
limit_act = 7.0
negative = -1e30


def round_offset(t):
    t = lax.div(t, SPLIT)
    odd = lax.rem(t, 2)
    return odd * lax.div(t + 1, 2) + (1 - odd) * lax.rem(Z - lax.div(t, 2), Z)


def y_offset(t, q):
    return lax.rem(t, SPLIT) * (SOURCES // 2) + lax.div(q, 2)


def wait_for(ref, sem):
    pltpu.make_async_copy(ref, ref, sem).wait()


def kernel(
    tok,
    gain,
    routes,
    rweights,
    qa,
    qb,
    lambdas,
    head_gain,
    ka_hbm,
    kb_hbm,
    v_hbm,
    wo_hbm,
    wg_hbm,
    wu_hbm,
    wd_hbm,
    out,
    mixer,
    wg,
    wu,
    wd,
    outgoing,
    gathered,
    partial,
    rs1,
    rs2,
    back,
    returned,
    hid,
    w_hi,
    w_lo,
    kv,
    wo,
    qp,
    peak,
    accum,
    heads,
    shares,
    passing,
    arrived,
    w_sem,
    kv_sem,
    disp_send,
    disp_recv,
    ag1_send,
    ag1_recv,
    ag2_send,
    ag2_recv,
    rs1_send,
    rs1_recv,
    rs2_send,
    rs2_recv,
    ret_send,
    ret_recv,
    kvz_send,
    kvz_recv,
    ky1_send,
    ky1_recv,
    ky2_send,
    ky2_recv,
    kp_send,
    kp_recv,
    mx_send,
    mx_recv,
):
    ep = lax.axis_index("ep")
    tp = lax.axis_index("tp")
    z = lax.div(ep, PLANE)
    mine = lax.rem(ep, PLANE)
    y, core = lax.div(mine, 2), lax.rem(mine, 2)
    x_left, x_right = lax.rem(tp + N_TP - 1, N_TP), lax.rem(tp + 1, N_TP)
    x_far = lax.rem(tp + 2, N_TP)
    left, right = (ep, x_left), (ep, x_right)
    lower, upper = pl.ds(0, TOKB // N_TP // 2), pl.ds(TOKB // N_TP // 2, TOKB // N_TP // 2)
    y_down, y_up, y_far = lax.rem(y + 3, 4), lax.rem(y + 1, 4), lax.rem(y + 2, 4)
    b_down, b_up, b_far = y_down * 2 + core, y_up * 2 + core, y_far * 2 + core
    up, down = (z * PLANE + b_up, tp), (z * PLANE + b_down, tp)
    peer = (z * PLANE + y * 2 + 1 - core, tp)
    rows = pl.ds(0, CAP)
    half_a, half_b = pl.ds(0, SOURCES // 2), pl.ds(SOURCES // 2, SOURCES // 2)
    one_core = pl.ds(0, PLANE // 2)

    def send(src, dst, send_sem, recv_sem, device):
        pltpu.make_async_remote_copy(
            src_ref=src,
            dst_ref=dst,
            send_sem=send_sem,
            recv_sem=recv_sem,
            device_id=device,
            device_id_type=MESH,
        ).start()

    barrier = pltpu.get_barrier_semaphore()

    def greet(e, carry):
        @pl.when(e != ep)
        def _():
            pl.semaphore_signal(barrier, inc=1, device_id=(e, tp), device_id_type=MESH)

        return carry

    lax.fori_loop(0, N_EP, greet, 0)
    for x in (x_left, x_right, x_far):
        pl.semaphore_signal(barrier, inc=1, device_id=(ep, x), device_id_type=MESH)

    own_kv = [
        pltpu.make_async_copy(ka_hbm, kv.at[z, mine, :, 0:128], kv_sem.at[0]),
        pltpu.make_async_copy(kb_hbm, kv.at[z, mine, :, 128:256], kv_sem.at[1]),
        pltpu.make_async_copy(v_hbm, kv.at[z, mine, :, 256:512], kv_sem.at[2]),
    ]
    weights = [
        pltpu.make_async_copy(wg_hbm.at[0], wg, w_sem.at[0]),
        pltpu.make_async_copy(wu_hbm.at[0], wu, w_sem.at[1]),
        pltpu.make_async_copy(wd_hbm.at[0], wd, w_sem.at[2]),
        pltpu.make_async_copy(wo_hbm, wo, w_sem.at[3]),
    ]
    for copy in own_kv + weights:
        copy.start()

    slot = lax.broadcasted_iota(jnp.int32, (EXPERTS * SLOT, TOKB), 0)
    expert, place = lax.div(slot, SLOT), lax.rem(slot, SLOT)
    first = routes[0:1, :] == expert
    second = routes[1:2, :] == expert
    member = jnp.where(first | second, 1.0, 0.0)
    earlier = lax.broadcasted_iota(jnp.int32, (TOKB, TOKB), 0) < lax.broadcasted_iota(
        jnp.int32, (TOKB, TOKB), 1
    )
    earlier = jnp.where(earlier, 1.0, 0.0).astype(BF16)
    count = jnp.dot(member.astype(BF16), earlier, preferred_element_type=F32)
    chosen = jnp.where(count == place.astype(F32), member, 0.0)
    inputs = tok[...].astype(F32)
    scale = lax.rsqrt(jnp.mean(inputs * inputs, axis=-1, keepdims=True) + eps)
    normed = (inputs * scale * gain[...]).astype(BF16)
    packed = jnp.dot(chosen.astype(BF16), normed, preferred_element_type=F32)
    outgoing[...] = packed.astype(BF16).reshape(EXPERTS, SLOT, D)

    pl.semaphore_wait(barrier, N_EP - 1 + N_TP - 1)

    def dispatch(t, carry):
        plane = lax.rem(z + round_offset(t), Z)

        def one(q, carry):
            e = plane * PLANE + lax.rem(y + y_offset(t, q), 4) * 2 + lax.rem(q, 2)
            src = outgoing.at[e, rows]
            dst = gathered.at[t, 0, lax.div(q, 2) * 2 + core, rows]

            @pl.when(e != ep)
            def _():
                send(src, dst, disp_send, disp_recv.at[t], (e, tp))

            @pl.when(e == ep)
            def _():
                pltpu.make_async_copy(src, dst, disp_recv.at[t]).start()

            return carry

        return lax.fori_loop(0, SOURCES, one, carry)

    lax.fori_loop(0, ROUNDS, dispatch, 0)

    for copy in own_kv:
        copy.wait()

    def kv_along_z(k, carry):
        @pl.when(z + k < Z)
        def _():
            block = kv.at[z, mine]
            send(block, block, kvz_send.at[k], kvz_recv.at[k], ((z + k) * PLANE + mine, tp))

        return carry

    lax.fori_loop(1, Z, kv_along_z, 0)

    weight = jnp.transpose(chosen * jnp.where(first, rweights[0:1, :], rweights[1:2, :]))
    high = weight.astype(BF16)
    w_hi[...] = high
    w_lo[...] = (weight - high.astype(F32)).astype(BF16)
    returned[:, CAP:SLOT, :] = jnp.zeros((EXPERTS, SLOT - CAP, D), BF16)

    group = 2 * TOKB
    peak[...] = jnp.full_like(peak, negative)
    accum[...] = jnp.zeros_like(accum)
    lane = lax.broadcasted_iota(jnp.int32, (TOKB, 128), 1)
    for which, source in enumerate((qa, qb)):
        for g in range(2):
            pair = source[:, g * 128 : (g + 1) * 128].astype(F32) * HEAD**-0.5
            for j in range(2):
                turned = pair if g == j else pltpu.roll(pair, 64, 1)
                part = jnp.where((lane >= 64) == (g == 1), turned, 0.0).astype(BF16)
                base = (which * 2 + g) * group + j * TOKB
                qp[base : base + TOKB, which * 128 : (which + 1) * 128] = part
                other = 1 - which
                qp[base : base + TOKB, other * 128 : (other + 1) * 128] = jnp.zeros_like(part)

    for copy in weights:
        copy.wait()

    def stage_spread(t):
        wait_for(gathered.at[t, 0, :, rows], disp_recv.at[t])
        own = gathered.at[t, 0, :, rows]
        send(own, gathered.at[t, 1, :, rows], ag1_send, ag1_recv.at[t, 0], right)
        send(own, gathered.at[t, 3, :, rows], ag1_send, ag1_recv.at[t, 1], left)

    def stage_forward(t):
        wait_for(gathered.at[t, 1, :, rows], ag1_recv.at[t, 0])
        send(
            gathered.at[t, 1, half_a, rows],
            gathered.at[t, 2, half_a, rows],
            ag2_send,
            ag2_recv.at[t, 0],
            right,
        )
        wait_for(gathered.at[t, 3, :, rows], ag1_recv.at[t, 1])
        send(
            gathered.at[t, 3, half_b, rows],
            gathered.at[t, 2, half_b, rows],
            ag2_send,
            ag2_recv.at[t, 1],
            left,
        )

    def stage_compute(t):
        wait_for(gathered.at[t, 2, half_a, rows], ag2_recv.at[t, 0])
        wait_for(gathered.at[t, 2, half_b, rows], ag2_recv.at[t, 1])
        for n in range(FFL // 256):
            cols = slice(n * 256, (n + 1) * 256)
            x = gathered[t].reshape(N_TP * SOURCES * SLOT, D)
            gate = jnp.dot(x, wg[:, cols], preferred_element_type=F32)
            up = jnp.dot(x, wu[:, cols], preferred_element_type=F32)
            capped = jnp.minimum(gate, limit_act)
            linear = jnp.clip(up, -limit_act, limit_act)
            act = capped * jax.nn.sigmoid(alpha_act * capped) * (linear + 1.0)
            hid[:, cols] = act.astype(BF16)

        def down_cols(n, carry):
            cols = pl.ds(pl.multiple_of(n * 512, 512), 512)
            part = jnp.dot(hid[...], wd[:, cols], preferred_element_type=F32)
            partial[t, :, :, :, cols] = part.astype(BF16).reshape(N_TP, SOURCES, SLOT, 512)
            return carry

        lax.fori_loop(0, D // 512, down_cols, 0)
        send(
            partial.at[t, 2, half_a, rows],
            rs1.at[t, 0, :, rows],
            rs1_send,
            rs1_recv.at[t, 0],
            right,
        )
        send(
            partial.at[t, 2, half_b, rows], rs1.at[t, 1, :, rows], rs1_send, rs1_recv.at[t, 1], left
        )
        send(
            partial.at[t, 3, half_b, rows],
            rs2.at[t, 0, half_b, rows],
            rs2_send,
            rs2_recv.at[t, 0, 1],
            right,
        )
        send(
            partial.at[t, 1, half_a, rows],
            rs2.at[t, 1, half_a, rows],
            rs2_send,
            rs2_recv.at[t, 1, 0],
            left,
        )

    def stage_add(t):
        wait_for(rs1.at[t, 0, :, rows], rs1_recv.at[t, 0])
        summed = partial[t, 3, half_a].astype(F32) + rs1[t, 0].astype(F32)
        partial[t, 3, half_a] = summed.astype(BF16)
        send(
            partial.at[t, 3, half_a, rows],
            rs2.at[t, 0, half_a, rows],
            rs2_send,
            rs2_recv.at[t, 0, 0],
            right,
        )
        wait_for(rs1.at[t, 1, :, rows], rs1_recv.at[t, 1])
        summed = partial[t, 1, half_b].astype(F32) + rs1[t, 1].astype(F32)
        partial[t, 1, half_b] = summed.astype(BF16)
        send(
            partial.at[t, 1, half_b, rows],
            rs2.at[t, 1, half_b, rows],
            rs2_send,
            rs2_recv.at[t, 1, 1],
            left,
        )

    def stage_return(t):
        for side in range(2):
            wait_for(rs2.at[t, side, half_a, rows], rs2_recv.at[t, side, 0])
            wait_for(rs2.at[t, side, half_b, rows], rs2_recv.at[t, side, 1])
        summed = partial[t, 0].astype(F32) + rs2[t, 0].astype(F32) + rs2[t, 1].astype(F32)
        back[t] = summed.astype(BF16)
        plane = lax.rem(z + Z - round_offset(t), Z)

        def one(q, carry):
            e = plane * PLANE + lax.rem(y + 4 - y_offset(t, q), 4) * 2 + lax.rem(q, 2)
            src = back.at[t, q, rows]
            dst = returned.at[ep, rows]

            @pl.when(e != ep)
            def _():
                send(src, dst, ret_send, ret_recv, (e, tp))

            @pl.when(e == ep)
            def _():
                pltpu.make_async_copy(src, dst, ret_recv).start()

            return carry

        lax.fori_loop(0, SOURCES, one, 0)

    def kv_spread(k):
        @pl.when(k > 0)
        def _():
            wait_for(kv.at[0, 0], kvz_recv.at[k])

        block = kv.at[z - k, mine]
        send(block, block, ky1_send.at[k], ky1_recv.at[k, 0], up)
        send(block, block, ky1_send.at[k], ky1_recv.at[k, 1], down)
        send(block, block, kp_send.at[k], kp_recv.at[k], peer)

    def kv_forward(k):
        near, far = pl.ds(0, TOKB // 2), pl.ds(TOKB // 2, TOKB // 2)
        block, part = kv.at[z - k, b_down], kv.at[z - k, b_down, near]
        wait_for(block, ky1_recv.at[k, 0])
        send(part, part, ky2_send.at[k], ky2_recv.at[k, 0], up)
        send(block, block, kp_send.at[k], kp_recv.at[k], peer)
        block, part = kv.at[z - k, b_up], kv.at[z - k, b_up, far]
        wait_for(block, ky1_recv.at[k, 1])
        send(part, part, ky2_send.at[k], ky2_recv.at[k, 1], down)
        send(block, block, kp_send.at[k], kp_recv.at[k], peer)

    def kv_share(k):
        block = kv.at[z - k, b_far]
        wait_for(kv.at[z - k, b_far, pl.ds(0, TOKB // 2)], ky2_recv.at[k, 0])
        wait_for(kv.at[z - k, b_far, pl.ds(TOKB // 2, TOKB // 2)], ky2_recv.at[k, 1])
        send(block, block, kp_send.at[k], kp_recv.at[k], peer)

    def visit(plane, masked):
        if masked:
            row = lax.broadcasted_iota(jnp.int32, (group, KBLOCK), 0)
            key = lax.broadcasted_iota(jnp.int32, (group, KBLOCK), 1)
            visible = key <= mine * TOKB + lax.rem(row, TOKB)
        for which in range(2):
            for g in range(2):
                at = slice((which * 2 + g) * group, (which * 2 + g + 1) * group)
                scores = lax.dot_general(
                    qp[at, :],
                    kv[plane, :, :, 0:256].reshape(KBLOCK, 256),
                    (((1,), (1,)), ((), ())),
                    preferred_element_type=F32,
                )
                if masked:
                    scores = jnp.where(visible, scores, negative)
                old = peak[at, :]
                new = jnp.maximum(old, jnp.max(scores, axis=1, keepdims=True))
                expo = jnp.exp(scores - new[:, 0:1])
                values = kv[plane, :, :, 256 + g * VDIM : 256 + (g + 1) * VDIM]
                values = values.reshape(KBLOCK, VDIM)
                values = jnp.concatenate([values, jnp.ones_like(values)], axis=1)
                mixed = jnp.dot(expo.astype(BF16), values, preferred_element_type=F32)
                fade = jnp.exp(old - new)
                accum[at, 0:VDIM] = accum[at, 0:VDIM] * fade + mixed[:, 0:VDIM]
                accum[at, VDIM:] = accum[at, VDIM:] * fade + mixed[:, VDIM:]
                peak[at, :] = new

    def kv_visit(k):
        wait_for(kv.at[0, one_core], kp_recv.at[k])

        @pl.when(k == 0)
        def _():
            visit(z, True)

        @pl.when(k > 0)
        def _():
            visit(z - k, False)

    def project():
        for g in range(2):
            for j in range(2):
                h = g * 2 + j
                a = slice(g * group + j * TOKB, g * group + (j + 1) * TOKB)
                b = slice((2 + g) * group + j * TOKB, (2 + g) * group + (j + 1) * TOKB)
                diff = accum[a, 0:VDIM] / accum[a, VDIM:] - lambdas[h] * (
                    accum[b, 0:VDIM] / accum[b, VDIM:]
                )
                scale = lax.rsqrt(jnp.mean(diff * diff, axis=-1, keepdims=True) + eps)
                heads[:, h * VDIM : (h + 1) * VDIM] = (diff * scale * head_gain[...]).astype(BF16)

        def columns(n, carry):
            cols = pl.ds(pl.multiple_of(n * 512, 512), 512)
            part = jnp.dot(heads[...], wo[:, cols], preferred_element_type=F32)
            shares[:, :, cols] = part.astype(BF16).reshape(N_TP, TOKB // N_TP, 512)
            return carry

        lax.fori_loop(0, D // 512, columns, 0)
        mix(0, shares.at[x_far, lower], passing.at[0], right)
        mix(1, shares.at[x_far, upper], passing.at[1], left)
        mix(2, shares.at[x_right, upper], arrived.at[0, upper], right)
        mix(3, shares.at[x_left, lower], arrived.at[1, lower], left)

    def mix(n, src, dst, device):
        send(src, dst, mx_send.at[n], mx_recv.at[n], device)

    def relay():
        wait_for(passing.at[0], mx_recv.at[0])
        summed = shares[x_right, lower].astype(F32) + passing[0].astype(F32)
        shares[x_right, lower] = summed.astype(BF16)
        mix(4, shares.at[x_right, lower], arrived.at[0, lower], right)
        wait_for(passing.at[1], mx_recv.at[1])
        summed = shares[x_left, upper].astype(F32) + passing[1].astype(F32)
        shares[x_left, upper] = summed.astype(BF16)
        mix(5, shares.at[x_left, upper], arrived.at[1, upper], left)

    stages = (stage_spread, stage_forward, stage_compute, stage_add, stage_return)
    kv_stages = (kv_spread, kv_forward, kv_share, kv_visit)
    project_tick = KV_LAG + Z + len(kv_stages) - 1

    def tick(i, carry):
        for lag in range(len(stages)):

            @pl.when((i >= lag) & (i - lag < ROUNDS))
            def _(lag=lag):
                stages[lag](i - lag)

        for lag in range(len(kv_stages)):
            k = i - KV_LAG - lag

            @pl.when((k >= 0) & (k < Z) & (k <= z))
            def _(lag=lag, k=k):
                kv_stages[lag](k)

        @pl.when(i == project_tick)
        def _():
            project()

        @pl.when(i == project_tick + 1)
        def _():
            relay()

        return carry

    lax.fori_loop(0, ROUNDS + len(stages) - 1, tick, 0)

    total = shares[tp].astype(F32)
    for n in range(2, 6):
        wait_for(passing.at[0], mx_recv.at[n])
    total = total + arrived[0].astype(F32) + arrived[1].astype(F32)
    mixer[...] = total.astype(BF16)

    wait_for(returned.at[:, rows], ret_recv)

    def combine(n, carry):
        cols = pl.ds(pl.multiple_of(n * 512, 512), 512)
        table = returned[:, :, cols].reshape(EXPERTS * SLOT, 512)
        total = jnp.dot(w_hi[...], table, preferred_element_type=F32)
        total = total + jnp.dot(w_lo[...], table, preferred_element_type=F32)
        out[:, cols] = total.astype(BF16)
        return carry

    lax.fori_loop(0, D // 512, combine, 0)

    some = pl.ds(0, N_EP - 1)
    wait_for(outgoing.at[some, rows], disp_send)
    wait_for(returned.at[some, rows], ret_send)
    wait_for(gathered.at[:, 0:2, :, rows], ag1_send)
    wait_for(back.at[:, :, rows], ag2_send)
    wait_for(back.at[:, :, rows], rs1_send)
    wait_for(gathered.at[:, 0:2, :, rows], rs2_send)
    for n in range(6):
        wait_for(passing.at[0], mx_send.at[n])

    def kv_sent(k, carry):
        @pl.when((k > 0) & (z + k < Z))
        def _():
            wait_for(kv.at[0, 0], kvz_send.at[k])

        @pl.when(k <= z)
        def _():
            wait_for(kv.at[0, 0:2], ky1_send.at[k])
            wait_for(kv.at[0, 0], ky2_send.at[k])
            wait_for(kv.at[0, one_core], kp_send.at[k])

        return carry

    lax.fori_loop(0, Z, kv_sent, 0)


def body(
    queries_a,
    queries_b,
    keys_a,
    keys_b,
    values,
    lambdas,
    head_gain,
    w_out,
    moe_tokens,
    moe_gain,
    routes,
    route_weights,
    w_gate,
    w_up,
    w_down,
):
    dma = pltpu.SemaphoreType.DMA
    vmem = pl.BlockSpec(memory_space=pltpu.VMEM)
    hbm = pl.BlockSpec(memory_space=pl.ANY)
    moe_out, mixer_out = pl.pallas_call(
        kernel,
        out_shape=(
            jax.ShapeDtypeStruct((TOKB, D), BF16),
            jax.ShapeDtypeStruct((TOKB // N_TP, D), BF16),
        ),
        in_specs=[vmem] * 6 + [pl.BlockSpec(memory_space=pltpu.SMEM), vmem] + [hbm] * 7,
        out_specs=(vmem, vmem),
        scratch_shapes=[
            pltpu.VMEM((D, FFL), BF16),
            pltpu.VMEM((D, FFL), BF16),
            pltpu.VMEM((FFL, D), BF16),
            pltpu.VMEM((EXPERTS, SLOT, D), BF16),
            pltpu.VMEM((ROUNDS, N_TP, SOURCES, SLOT, D), BF16),
            pltpu.VMEM((ROUNDS, N_TP, SOURCES, SLOT, D), BF16),
            pltpu.VMEM((ROUNDS, 2, SOURCES // 2, SLOT, D), BF16),
            pltpu.VMEM((ROUNDS, 2, SOURCES, SLOT, D), BF16),
            pltpu.VMEM((ROUNDS, SOURCES, SLOT, D), BF16),
            pltpu.VMEM((EXPERTS, SLOT, D), BF16),
            pltpu.VMEM((N_TP * SOURCES * SLOT, FFL), BF16),
            pltpu.VMEM((TOKB, EXPERTS * SLOT), BF16),
            pltpu.VMEM((TOKB, EXPERTS * SLOT), BF16),
            pltpu.VMEM((Z, PLANE, TOKB, 512), BF16),
            pltpu.VMEM((512, D), BF16),
            pltpu.VMEM((8 * TOKB, 256), BF16),
            pltpu.VMEM((8 * TOKB, 128), F32),
            pltpu.VMEM((8 * TOKB, 256), F32),
            pltpu.VMEM((TOKB, 512), BF16),
            pltpu.VMEM((N_TP, TOKB // N_TP, D), BF16),
            pltpu.VMEM((2, TOKB // N_TP // 2, D), BF16),
            pltpu.VMEM((2, TOKB // N_TP, D), BF16),
            dma((4,)),
            dma((3,)),
            dma,
            dma((ROUNDS,)),
            dma,
            dma((ROUNDS, 2)),
            dma,
            dma((ROUNDS, 2)),
            dma,
            dma((ROUNDS, 2)),
            dma,
            dma((ROUNDS, 2, 2)),
            dma,
            dma,
            dma((Z,)),
            dma((Z,)),
            dma((Z,)),
            dma((Z, 2)),
            dma((Z,)),
            dma((Z, 2)),
            dma((Z,)),
            dma((Z,)),
            dma((6,)),
            dma((6,)),
        ],
        compiler_params=pltpu.CompilerParams(
            collective_id=0, has_side_effects=True, vmem_limit_bytes=60 * 1024 * 1024
        ),
        name="layer",
    )(
        moe_tokens,
        moe_gain.reshape(1, D),
        routes.T,
        route_weights.T,
        queries_a,
        queries_b,
        lambdas,
        head_gain.reshape(1, VDIM),
        keys_a,
        keys_b,
        values,
        w_out,
        w_gate,
        w_up,
        w_down,
    )
    return (mixer_out, moe_out)


def solution(mesh):
    return jax.shard_map(
        body,
        mesh=mesh,
        in_specs=(
            P("ep", "tp"),
            P("ep", "tp"),
            P("ep", "tp"),
            P("ep", "tp"),
            P("ep", "tp"),
            P("tp"),
            P(),
            P("tp", None),
            P(("ep", "tp"), None),
            P(),
            P(("ep", "tp"), None),
            P(("ep", "tp"), None),
            P("ep", None, "tp"),
            P("ep", None, "tp"),
            P("ep", "tp", None),
        ),
        out_specs=(P(("ep", "tp"), None), P(("ep", "tp"), None)),
        check_vma=False,
    )
```

```python
import jax
import jax.numpy as jnp
from jax import lax
from jax.experimental import pallas as pl
from jax.experimental.pallas import tpu as pltpu
from jax.sharding import PartitionSpec as P

MESH = pl.DeviceIdType.MESH
BF16 = jnp.bfloat16
F32 = jnp.float32

D = 2048
HEAD = 64
VDIM = 128
N_EP = 64
N_TP = 4
PLANE = 8
Z = 8
SPLIT = 2
ROUNDS = Z * SPLIT
SOURCES = PLANE // SPLIT
CAP = 6
SLOT = 8
EXPERTS = 64
TOKB = 128
FFL = 512
KBLOCK = 1024
LAG = 2
KV_STEP = SPLIT // 2
KV_LAG = 3 * SPLIT
SETUP_TICK = 2 * SPLIT

eps = 1e-05
alpha_act = 1.702
limit_act = 7.0
negative = -1e30


def z_offset(n):
    odd = lax.rem(n, 2)
    return odd * lax.div(n + 1, 2) + (1 - odd) * lax.rem(Z - lax.div(n, 2), Z)


def round_offset(t):
    return z_offset(lax.rem(lax.div(t + SPLIT // 2, SPLIT), Z))


def y_offset(t, q):
    return lax.rem(t, SPLIT) * (SOURCES // 2) + lax.div(q, 2)


def wait_for(ref, sem):
    pltpu.make_async_copy(ref, ref, sem).wait()


def kernel(
    tok,
    gain,
    routes,
    rweights,
    qa,
    qb,
    lambdas,
    head_gain,
    ka_hbm,
    kb_hbm,
    v_hbm,
    wo_hbm,
    wg_hbm,
    wu_hbm,
    wd_hbm,
    out,
    mixer,
    wg,
    wu,
    wd,
    picks,
    normed,
    outgoing,
    gathered,
    partial,
    rs1,
    rs2,
    back,
    returned,
    hid,
    w_hi,
    w_lo,
    kv,
    wo,
    qp,
    peak,
    accum,
    heads,
    shares,
    passing,
    arrived,
    w_sem,
    kv_sem,
    disp_send,
    disp_recv,
    ag1_send,
    ag1_recv,
    ag2_send,
    ag2_recv,
    rs1_send,
    rs1_recv,
    rs2_send,
    rs2_recv,
    ret_send,
    ret_recv,
    kvz_send,
    kvz_recv,
    ky1_send,
    ky1_recv,
    ky2_send,
    ky2_recv,
    kp_send,
    kp_recv,
    mx_send,
    mx_recv,
):
    ep = lax.axis_index("ep")
    tp = lax.axis_index("tp")
    z = lax.div(ep, PLANE)
    mine = lax.rem(ep, PLANE)
    y, core = lax.div(mine, 2), lax.rem(mine, 2)
    x_left, x_right = lax.rem(tp + N_TP - 1, N_TP), lax.rem(tp + 1, N_TP)
    x_far = lax.rem(tp + 2, N_TP)
    left, right = (ep, x_left), (ep, x_right)
    lower, upper = pl.ds(0, TOKB // N_TP // 2), pl.ds(TOKB // N_TP // 2, TOKB // N_TP // 2)
    y_down, y_up, y_far = lax.rem(y + 3, 4), lax.rem(y + 1, 4), lax.rem(y + 2, 4)
    b_down, b_up, b_far = y_down * 2 + core, y_up * 2 + core, y_far * 2 + core
    up, down = (z * PLANE + b_up, tp), (z * PLANE + b_down, tp)
    peer = (z * PLANE + y * 2 + 1 - core, tp)
    rows = pl.ds(0, CAP)
    half_a, half_b = pl.ds(0, SOURCES // 2), pl.ds(SOURCES // 2, SOURCES // 2)
    one_core = pl.ds(0, PLANE // 2)

    def send(src, dst, send_sem, recv_sem, device):
        pltpu.make_async_remote_copy(
            src_ref=src,
            dst_ref=dst,
            send_sem=send_sem,
            recv_sem=recv_sem,
            device_id=device,
            device_id_type=MESH,
        ).start()

    barrier = pltpu.get_barrier_semaphore()

    def greet(e, carry):
        @pl.when(e != ep)
        def _():
            pl.semaphore_signal(barrier, inc=1, device_id=(e, tp), device_id_type=MESH)

        return carry

    lax.fori_loop(0, N_EP, greet, 0)
    for x in (x_left, x_right, x_far):
        pl.semaphore_signal(barrier, inc=1, device_id=(ep, x), device_id_type=MESH)

    own_kv = [
        pltpu.make_async_copy(ka_hbm, kv.at[z, mine, :, 0:128], kv_sem.at[0]),
        pltpu.make_async_copy(kb_hbm, kv.at[z, mine, :, 128:256], kv_sem.at[1]),
        pltpu.make_async_copy(v_hbm, kv.at[z, mine, :, 256:512], kv_sem.at[2]),
    ]
    weights = [
        pltpu.make_async_copy(wg_hbm.at[0], wg, w_sem.at[0]),
        pltpu.make_async_copy(wu_hbm.at[0], wu, w_sem.at[1]),
        pltpu.make_async_copy(wd_hbm.at[0], wd, w_sem.at[2]),
        pltpu.make_async_copy(wo_hbm, wo, w_sem.at[3]),
    ]
    for copy in own_kv + weights:
        copy.start()

    slot = lax.broadcasted_iota(jnp.int32, (EXPERTS * SLOT, TOKB), 0)
    expert, place = lax.div(slot, SLOT), lax.rem(slot, SLOT)
    first = routes[0:1, :] == expert
    second = routes[1:2, :] == expert
    member = jnp.where(first | second, 1.0, 0.0)
    earlier = lax.broadcasted_iota(jnp.int32, (TOKB, TOKB), 0) < lax.broadcasted_iota(
        jnp.int32, (TOKB, TOKB), 1
    )
    earlier = jnp.where(earlier, 1.0, 0.0).astype(BF16)
    count = jnp.dot(member.astype(BF16), earlier, preferred_element_type=F32)
    picks[...] = jnp.where(count == place.astype(F32), member, 0.0).astype(BF16)
    inputs = tok[...].astype(F32)
    scale = lax.rsqrt(jnp.mean(inputs * inputs, axis=-1, keepdims=True) + eps)
    normed[...] = (inputs * scale * gain[...]).astype(BF16)
    pl.semaphore_wait(barrier, N_EP - 1 + N_TP - 1)

    def dispatch(t, carry):
        plane = lax.rem(z + round_offset(t), Z)

        def one(q, carry):
            e = plane * PLANE + lax.rem(y + y_offset(t, q), 4) * 2 + lax.rem(q, 2)
            src = outgoing.at[e, rows]
            dst = gathered.at[t, 0, lax.div(q, 2) * 2 + core, rows]

            @pl.when(e != ep)
            def _():
                send(src, dst, disp_send, disp_recv.at[t], (e, tp))

            @pl.when(e == ep)
            def _():
                pltpu.make_async_copy(src, dst, disp_recv.at[t]).start()

            return carry

        return lax.fori_loop(0, SOURCES, one, carry)

    def pack(n):
        plane = lax.rem(z + z_offset(n), Z)
        slots = pl.ds(pl.multiple_of(plane * PLANE * SLOT, PLANE * SLOT), PLANE * SLOT)
        packed = jnp.dot(picks[slots, :], normed[...], preferred_element_type=F32)
        experts = pl.ds(plane * PLANE, PLANE)
        outgoing[experts] = packed.astype(BF16).reshape(PLANE, SLOT, D)

    def pack_and_send(n, carry):
        pack(n)
        begin = jnp.maximum(n * SPLIT - SPLIT // 2, 0)
        return lax.fori_loop(begin, n * SPLIT + SPLIT // 2, dispatch, carry)

    lax.fori_loop(0, Z, pack_and_send, 0)
    lax.fori_loop(ROUNDS - SPLIT // 2, ROUNDS, dispatch, 0)

    for copy in own_kv:
        copy.wait()

    def kv_along_z(k, carry):
        @pl.when(z + k < Z)
        def _():
            block = kv.at[z, mine]
            send(block, block, kvz_send.at[k], kvz_recv.at[k], ((z + k) * PLANE + mine, tp))

        return carry

    lax.fori_loop(1, Z, kv_along_z, 0)

    group = 2 * TOKB

    for copy in weights:
        copy.wait()

    def setup():
        first = routes[0:1, :] == lax.div(
            lax.broadcasted_iota(jnp.int32, (EXPERTS * SLOT, TOKB), 0), SLOT
        )
        weight = jnp.where(first, rweights[0:1, :], rweights[1:2, :])
        weight = jnp.transpose(picks[...].astype(F32) * weight)
        high = weight.astype(BF16)
        w_hi[...] = high
        w_lo[...] = (weight - high.astype(F32)).astype(BF16)
        returned[:, CAP:SLOT, :] = jnp.zeros((EXPERTS, SLOT - CAP, D), BF16)

        peak[...] = jnp.full_like(peak, negative)
        accum[...] = jnp.zeros_like(accum)
        lane = lax.broadcasted_iota(jnp.int32, (TOKB, 128), 1)
        for which, source in enumerate((qa, qb)):
            for g in range(2):
                pair = source[:, g * 128 : (g + 1) * 128].astype(F32) * HEAD**-0.5
                for j in range(2):
                    turned = pair if g == j else pltpu.roll(pair, 64, 1)
                    part = jnp.where((lane >= 64) == (g == 1), turned, 0.0).astype(BF16)
                    base = (which * 2 + g) * group + j * TOKB
                    qp[base : base + TOKB, which * 128 : (which + 1) * 128] = part
                    other = 1 - which
                    qp[base : base + TOKB, other * 128 : (other + 1) * 128] = jnp.zeros_like(part)

    def stage_spread(t):
        wait_for(gathered.at[t, 0, :, rows], disp_recv.at[t])
        own = gathered.at[t, 0, :, rows]
        send(own, gathered.at[t, 1, :, rows], ag1_send, ag1_recv.at[t, 0], right)
        send(own, gathered.at[t, 3, :, rows], ag1_send, ag1_recv.at[t, 1], left)

    def stage_forward(t):
        wait_for(gathered.at[t, 1, :, rows], ag1_recv.at[t, 0])
        send(
            gathered.at[t, 1, half_a, rows],
            gathered.at[t, 2, half_a, rows],
            ag2_send,
            ag2_recv.at[t, 0],
            right,
        )
        wait_for(gathered.at[t, 3, :, rows], ag1_recv.at[t, 1])
        send(
            gathered.at[t, 3, half_b, rows],
            gathered.at[t, 2, half_b, rows],
            ag2_send,
            ag2_recv.at[t, 1],
            left,
        )

    def stage_compute(t):
        wait_for(gathered.at[t, 2, half_a, rows], ag2_recv.at[t, 0])
        wait_for(gathered.at[t, 2, half_b, rows], ag2_recv.at[t, 1])
        for n in range(FFL // 256):
            cols = slice(n * 256, (n + 1) * 256)
            x = gathered[t].reshape(N_TP * SOURCES * SLOT, D)
            gate = jnp.dot(x, wg[:, cols], preferred_element_type=F32)
            up = jnp.dot(x, wu[:, cols], preferred_element_type=F32)
            capped = jnp.minimum(gate, limit_act)
            linear = jnp.clip(up, -limit_act, limit_act)
            act = capped * jax.nn.sigmoid(alpha_act * capped) * (linear + 1.0)
            hid[:, cols] = act.astype(BF16)

        def down_cols(n, carry):
            cols = pl.ds(pl.multiple_of(n * 512, 512), 512)
            part = jnp.dot(hid[...], wd[:, cols], preferred_element_type=F32)
            partial[t, :, :, :, cols] = part.astype(BF16).reshape(N_TP, SOURCES, SLOT, 512)
            return carry

        lax.fori_loop(0, D // 512, down_cols, 0)
        send(
            partial.at[t, 2, half_a, rows],
            rs1.at[t, 0, :, rows],
            rs1_send,
            rs1_recv.at[t, 0],
            right,
        )
        send(
            partial.at[t, 2, half_b, rows], rs1.at[t, 1, :, rows], rs1_send, rs1_recv.at[t, 1], left
        )
        send(
            partial.at[t, 3, half_b, rows],
            rs2.at[t, 0, half_b, rows],
            rs2_send,
            rs2_recv.at[t, 0, 1],
            right,
        )
        send(
            partial.at[t, 1, half_a, rows],
            rs2.at[t, 1, half_a, rows],
            rs2_send,
            rs2_recv.at[t, 1, 0],
            left,
        )

    def stage_add(t):
        wait_for(rs1.at[t, 0, :, rows], rs1_recv.at[t, 0])
        summed = partial[t, 3, half_a].astype(F32) + rs1[t, 0].astype(F32)
        partial[t, 3, half_a] = summed.astype(BF16)
        send(
            partial.at[t, 3, half_a, rows],
            rs2.at[t, 0, half_a, rows],
            rs2_send,
            rs2_recv.at[t, 0, 0],
            right,
        )
        wait_for(rs1.at[t, 1, :, rows], rs1_recv.at[t, 1])
        summed = partial[t, 1, half_b].astype(F32) + rs1[t, 1].astype(F32)
        partial[t, 1, half_b] = summed.astype(BF16)
        send(
            partial.at[t, 1, half_b, rows],
            rs2.at[t, 1, half_b, rows],
            rs2_send,
            rs2_recv.at[t, 1, 1],
            left,
        )

    def stage_return(t):
        for side in range(2):
            wait_for(rs2.at[t, side, half_a, rows], rs2_recv.at[t, side, 0])
            wait_for(rs2.at[t, side, half_b, rows], rs2_recv.at[t, side, 1])
        summed = partial[t, 0].astype(F32) + rs2[t, 0].astype(F32) + rs2[t, 1].astype(F32)
        back[t] = summed.astype(BF16)
        plane = lax.rem(z + Z - round_offset(t), Z)

        def one(q, carry):
            e = plane * PLANE + lax.rem(y + 4 - y_offset(t, q), 4) * 2 + lax.rem(q, 2)
            src = back.at[t, q, rows]
            dst = returned.at[ep, rows]

            @pl.when(e != ep)
            def _():
                send(src, dst, ret_send, ret_recv, (e, tp))

            @pl.when(e == ep)
            def _():
                pltpu.make_async_copy(src, dst, ret_recv).start()

            return carry

        lax.fori_loop(0, SOURCES, one, 0)

    def kv_spread(k):
        @pl.when(k > 0)
        def _():
            wait_for(kv.at[0, 0], kvz_recv.at[k])

        block = kv.at[z - k, mine]
        send(block, block, ky1_send.at[k], ky1_recv.at[k, 0], up)
        send(block, block, ky1_send.at[k], ky1_recv.at[k, 1], down)
        send(block, block, kp_send.at[k], kp_recv.at[k], peer)

    def kv_forward(k):
        near, far = pl.ds(0, TOKB // 2), pl.ds(TOKB // 2, TOKB // 2)
        block, part = kv.at[z - k, b_down], kv.at[z - k, b_down, near]
        wait_for(block, ky1_recv.at[k, 0])
        send(part, part, ky2_send.at[k], ky2_recv.at[k, 0], up)
        send(block, block, kp_send.at[k], kp_recv.at[k], peer)
        block, part = kv.at[z - k, b_up], kv.at[z - k, b_up, far]
        wait_for(block, ky1_recv.at[k, 1])
        send(part, part, ky2_send.at[k], ky2_recv.at[k, 1], down)
        send(block, block, kp_send.at[k], kp_recv.at[k], peer)

    def kv_share(k):
        block = kv.at[z - k, b_far]
        wait_for(kv.at[z - k, b_far, pl.ds(0, TOKB // 2)], ky2_recv.at[k, 0])
        wait_for(kv.at[z - k, b_far, pl.ds(TOKB // 2, TOKB // 2)], ky2_recv.at[k, 1])
        send(block, block, kp_send.at[k], kp_recv.at[k], peer)

    def visit(plane, masked):
        if masked:
            row = lax.broadcasted_iota(jnp.int32, (group, KBLOCK), 0)
            key = lax.broadcasted_iota(jnp.int32, (group, KBLOCK), 1)
            visible = key <= mine * TOKB + lax.rem(row, TOKB)
        for which in range(2):
            for g in range(2):
                at = slice((which * 2 + g) * group, (which * 2 + g + 1) * group)
                scores = lax.dot_general(
                    qp[at, :],
                    kv[plane, :, :, 0:256].reshape(KBLOCK, 256),
                    (((1,), (1,)), ((), ())),
                    preferred_element_type=F32,
                )
                if masked:
                    scores = jnp.where(visible, scores, negative)
                old = peak[at, :]
                new = jnp.maximum(old, jnp.max(scores, axis=1, keepdims=True))
                expo = jnp.exp(scores - new[:, 0:1])
                values = kv[plane, :, :, 256 + g * VDIM : 256 + (g + 1) * VDIM]
                values = values.reshape(KBLOCK, VDIM)
                values = jnp.concatenate([values, jnp.ones_like(values)], axis=1)
                mixed = jnp.dot(expo.astype(BF16), values, preferred_element_type=F32)
                fade = jnp.exp(old - new)
                accum[at, 0:VDIM] = accum[at, 0:VDIM] * fade + mixed[:, 0:VDIM]
                accum[at, VDIM:] = accum[at, VDIM:] * fade + mixed[:, VDIM:]
                peak[at, :] = new

    def kv_visit(k):
        wait_for(kv.at[0, one_core], kp_recv.at[k])

        @pl.when(k == 0)
        def _():
            visit(z, True)

        @pl.when(k > 0)
        def _():
            visit(z - k, False)

    def project():
        for g in range(2):
            for j in range(2):
                h = g * 2 + j
                a = slice(g * group + j * TOKB, g * group + (j + 1) * TOKB)
                b = slice((2 + g) * group + j * TOKB, (2 + g) * group + (j + 1) * TOKB)
                diff = accum[a, 0:VDIM] / accum[a, VDIM:] - lambdas[h] * (
                    accum[b, 0:VDIM] / accum[b, VDIM:]
                )
                scale = lax.rsqrt(jnp.mean(diff * diff, axis=-1, keepdims=True) + eps)
                heads[:, h * VDIM : (h + 1) * VDIM] = (diff * scale * head_gain[...]).astype(BF16)

        def columns(n, carry):
            cols = pl.ds(pl.multiple_of(n * 512, 512), 512)
            part = jnp.dot(heads[...], wo[:, cols], preferred_element_type=F32)
            shares[:, :, cols] = part.astype(BF16).reshape(N_TP, TOKB // N_TP, 512)
            return carry

        lax.fori_loop(0, D // 512, columns, 0)

    def mix(n, src, dst, device):
        send(src, dst, mx_send.at[n], mx_recv.at[n], device)

    def share_out():
        mix(0, shares.at[x_far, lower], passing.at[0], right)
        mix(1, shares.at[x_far, upper], passing.at[1], left)
        mix(2, shares.at[x_right, upper], arrived.at[0, upper], right)
        mix(3, shares.at[x_left, lower], arrived.at[1, lower], left)

    def relay():
        wait_for(passing.at[0], mx_recv.at[0])
        summed = shares[x_right, lower].astype(F32) + passing[0].astype(F32)
        shares[x_right, lower] = summed.astype(BF16)
        mix(4, shares.at[x_right, lower], arrived.at[0, lower], right)
        wait_for(passing.at[1], mx_recv.at[1])
        summed = shares[x_left, upper].astype(F32) + passing[1].astype(F32)
        shares[x_left, upper] = summed.astype(BF16)
        mix(5, shares.at[x_left, upper], arrived.at[1, upper], left)

    stages = (stage_spread, stage_forward, stage_compute, stage_add, stage_return)
    kv_stages = (kv_spread, kv_forward, kv_share, kv_visit)
    last_tick = ROUNDS - 1 + (len(stages) - 1) * LAG

    def tick(i, carry):
        for n in range(len(stages)):
            t = i - n * LAG

            @pl.when((t >= 0) & (t < ROUNDS))
            def _(n=n, t=t):
                stages[n](t)

        for n in range(len(kv_stages)):
            step = i - KV_LAG
            k = lax.div(step, KV_STEP) - n

            @pl.when((step >= 0) & (lax.rem(step, KV_STEP) == 0) & (k >= 0) & (k < Z) & (k <= z))
            def _(n=n, k=k):
                kv_stages[n](k)

        @pl.when(i == SETUP_TICK)
        def _():
            setup()

        @pl.when(i == KV_LAG + (Z + len(kv_stages) - 1) * KV_STEP)
        def _():
            project()

        @pl.when(i == last_tick - LAG)
        def _():
            share_out()

        @pl.when(i == last_tick)
        def _():
            relay()

        return carry

    lax.fori_loop(0, last_tick + 1, tick, 0)

    wait_for(returned.at[:, rows], ret_recv)

    def combine(n, carry):
        cols = pl.ds(pl.multiple_of(n * 512, 512), 512)
        table = returned[:, :, cols].reshape(EXPERTS * SLOT, 512)
        total = jnp.dot(w_hi[...], table, preferred_element_type=F32)
        total = total + jnp.dot(w_lo[...], table, preferred_element_type=F32)
        out[:, cols] = total.astype(BF16)
        return carry

    lax.fori_loop(0, D // 512, combine, 0)

    total = shares[tp].astype(F32)
    for n in range(2, 6):
        wait_for(passing.at[0], mx_recv.at[n])
    total = total + arrived[0].astype(F32) + arrived[1].astype(F32)
    mixer[...] = total.astype(BF16)

    some = pl.ds(0, N_EP - 1)
    wait_for(outgoing.at[some, rows], disp_send)
    wait_for(returned.at[some, rows], ret_send)
    wait_for(gathered.at[:, 0:2, :, rows], ag1_send)
    wait_for(back.at[:, :, rows], ag2_send)
    wait_for(back.at[:, :, rows], rs1_send)
    wait_for(gathered.at[:, 0:2, :, rows], rs2_send)
    for n in range(6):
        wait_for(passing.at[0], mx_send.at[n])

    def kv_sent(k, carry):
        @pl.when((k > 0) & (z + k < Z))
        def _():
            wait_for(kv.at[0, 0], kvz_send.at[k])

        @pl.when(k <= z)
        def _():
            wait_for(kv.at[0, 0:2], ky1_send.at[k])
            wait_for(kv.at[0, 0], ky2_send.at[k])
            wait_for(kv.at[0, one_core], kp_send.at[k])

        return carry

    lax.fori_loop(0, Z, kv_sent, 0)


def body(
    queries_a,
    queries_b,
    keys_a,
    keys_b,
    values,
    lambdas,
    head_gain,
    w_out,
    moe_tokens,
    moe_gain,
    routes,
    route_weights,
    w_gate,
    w_up,
    w_down,
):
    dma = pltpu.SemaphoreType.DMA
    vmem = pl.BlockSpec(memory_space=pltpu.VMEM)
    hbm = pl.BlockSpec(memory_space=pl.ANY)
    moe_out, mixer_out = pl.pallas_call(
        kernel,
        out_shape=(
            jax.ShapeDtypeStruct((TOKB, D), BF16),
            jax.ShapeDtypeStruct((TOKB // N_TP, D), BF16),
        ),
        in_specs=[vmem] * 6 + [pl.BlockSpec(memory_space=pltpu.SMEM), vmem] + [hbm] * 7,
        out_specs=(vmem, vmem),
        scratch_shapes=[
            pltpu.VMEM((D, FFL), BF16),
            pltpu.VMEM((D, FFL), BF16),
            pltpu.VMEM((FFL, D), BF16),
            pltpu.VMEM((EXPERTS * SLOT, TOKB), BF16),
            pltpu.VMEM((TOKB, D), BF16),
            pltpu.VMEM((EXPERTS, SLOT, D), BF16),
            pltpu.VMEM((ROUNDS, N_TP, SOURCES, SLOT, D), BF16),
            pltpu.VMEM((ROUNDS, N_TP, SOURCES, SLOT, D), BF16),
            pltpu.VMEM((ROUNDS, 2, SOURCES // 2, SLOT, D), BF16),
            pltpu.VMEM((ROUNDS, 2, SOURCES, SLOT, D), BF16),
            pltpu.VMEM((ROUNDS, SOURCES, SLOT, D), BF16),
            pltpu.VMEM((EXPERTS, SLOT, D), BF16),
            pltpu.VMEM((N_TP * SOURCES * SLOT, FFL), BF16),
            pltpu.VMEM((TOKB, EXPERTS * SLOT), BF16),
            pltpu.VMEM((TOKB, EXPERTS * SLOT), BF16),
            pltpu.VMEM((Z, PLANE, TOKB, 512), BF16),
            pltpu.VMEM((512, D), BF16),
            pltpu.VMEM((8 * TOKB, 256), BF16),
            pltpu.VMEM((8 * TOKB, 128), F32),
            pltpu.VMEM((8 * TOKB, 256), F32),
            pltpu.VMEM((TOKB, 512), BF16),
            pltpu.VMEM((N_TP, TOKB // N_TP, D), BF16),
            pltpu.VMEM((2, TOKB // N_TP // 2, D), BF16),
            pltpu.VMEM((2, TOKB // N_TP, D), BF16),
            dma((4,)),
            dma((3,)),
            dma,
            dma((ROUNDS,)),
            dma,
            dma((ROUNDS, 2)),
            dma,
            dma((ROUNDS, 2)),
            dma,
            dma((ROUNDS, 2)),
            dma,
            dma((ROUNDS, 2, 2)),
            dma,
            dma,
            dma((Z,)),
            dma((Z,)),
            dma((Z,)),
            dma((Z, 2)),
            dma((Z,)),
            dma((Z, 2)),
            dma((Z,)),
            dma((Z,)),
            dma((6,)),
            dma((6,)),
        ],
        compiler_params=pltpu.CompilerParams(
            collective_id=0, has_side_effects=True, vmem_limit_bytes=60 * 1024 * 1024
        ),
        name="layer",
    )(
        moe_tokens,
        moe_gain.reshape(1, D),
        routes.T,
        route_weights.T,
        queries_a,
        queries_b,
        lambdas,
        head_gain.reshape(1, VDIM),
        keys_a,
        keys_b,
        values,
        w_out,
        w_gate,
        w_up,
        w_down,
    )
    return (mixer_out, moe_out)


def solution(mesh):
    return jax.shard_map(
        body,
        mesh=mesh,
        in_specs=(
            P("ep", "tp"),
            P("ep", "tp"),
            P("ep", "tp"),
            P("ep", "tp"),
            P("ep", "tp"),
            P("tp"),
            P(),
            P("tp", None),
            P(("ep", "tp"), None),
            P(),
            P(("ep", "tp"), None),
            P(("ep", "tp"), None),
            P("ep", None, "tp"),
            P("ep", None, "tp"),
            P("ep", "tp", None),
        ),
        out_specs=(P(("ep", "tp"), None), P(("ep", "tp"), None)),
        check_vma=False,
    )
```

```python
import jax
import jax.numpy as jnp
from jax import lax
from jax.experimental import pallas as pl
from jax.experimental.pallas import tpu as pltpu
from jax.sharding import PartitionSpec as P

MESH = pl.DeviceIdType.MESH
BF16 = jnp.bfloat16
F32 = jnp.float32

D = 2048
HEAD = 64
VDIM = 128
N_EP = 64
N_TP = 4
PLANE = 8
Z = 8
SPLIT = 2
ROUNDS = Z * SPLIT
SOURCES = PLANE // SPLIT
CAP = 6
SLOT = 8
EXPERTS = 64
TOKB = 128
FFL = 512
KBLOCK = 1024
LAG = 1
KV_STEP = SPLIT // 2
KV_LAG = 3 * SPLIT + 1
SETUP_TICK = 2 * SPLIT

eps = 1e-05
alpha_act = 1.702
limit_act = 7.0
negative = -1e30


def z_offset(n):
    odd = lax.rem(n, 2)
    return odd * lax.div(n + 1, 2) + (1 - odd) * lax.rem(Z - lax.div(n, 2), Z)


def round_offset(t):
    return z_offset(lax.rem(lax.div(t + SPLIT // 2, SPLIT), Z))


def y_offset(t, q):
    return lax.rem(t, SPLIT) * (SOURCES // 2) + lax.div(q, 2)


def wait_for(ref, sem):
    pltpu.make_async_copy(ref, ref, sem).wait()


def kernel(
    tok,
    gain,
    routes,
    rweights,
    qa,
    qb,
    lambdas,
    head_gain,
    ka_hbm,
    kb_hbm,
    v_hbm,
    wo_hbm,
    wg_hbm,
    wu_hbm,
    wd_hbm,
    out,
    mixer,
    wg,
    wu,
    wd,
    picks,
    normed,
    outgoing,
    gathered,
    partial,
    rs1,
    rs2,
    back,
    returned,
    hid,
    w_hi,
    w_lo,
    kv,
    wo,
    qp,
    peak,
    accum,
    heads,
    shares,
    passing,
    arrived,
    w_sem,
    kv_sem,
    disp_send,
    disp_recv,
    ag1_send,
    ag1_recv,
    ag2_send,
    ag2_recv,
    rs1_send,
    rs1_recv,
    rs2_send,
    rs2_recv,
    ret_send,
    ret_recv,
    kvz_send,
    kvz_recv,
    ky1_send,
    ky1_recv,
    ky2_send,
    ky2_recv,
    kp_send,
    kp_recv,
    mx_send,
    mx_recv,
):
    ep = lax.axis_index("ep")
    tp = lax.axis_index("tp")
    z = lax.div(ep, PLANE)
    mine = lax.rem(ep, PLANE)
    y, core = lax.div(mine, 2), lax.rem(mine, 2)
    x_left, x_right = lax.rem(tp + N_TP - 1, N_TP), lax.rem(tp + 1, N_TP)
    x_far = lax.rem(tp + 2, N_TP)
    left, right = (ep, x_left), (ep, x_right)
    lower, upper = pl.ds(0, TOKB // N_TP // 2), pl.ds(TOKB // N_TP // 2, TOKB // N_TP // 2)
    y_down, y_up, y_far = lax.rem(y + 3, 4), lax.rem(y + 1, 4), lax.rem(y + 2, 4)
    b_down, b_up, b_far = y_down * 2 + core, y_up * 2 + core, y_far * 2 + core
    up, down = (z * PLANE + b_up, tp), (z * PLANE + b_down, tp)
    peer = (z * PLANE + y * 2 + 1 - core, tp)
    rows = pl.ds(0, CAP)
    half_a, half_b = pl.ds(0, SOURCES // 2), pl.ds(SOURCES // 2, SOURCES // 2)
    one_core = pl.ds(0, PLANE // 2)

    def send(src, dst, send_sem, recv_sem, device):
        pltpu.make_async_remote_copy(
            src_ref=src,
            dst_ref=dst,
            send_sem=send_sem,
            recv_sem=recv_sem,
            device_id=device,
            device_id_type=MESH,
        ).start()

    barrier = pltpu.get_barrier_semaphore()

    def greet(e, carry):
        @pl.when(e != ep)
        def _():
            pl.semaphore_signal(barrier, inc=1, device_id=(e, tp), device_id_type=MESH)

        return carry

    lax.fori_loop(0, N_EP, greet, 0)
    for x in (x_left, x_right, x_far):
        pl.semaphore_signal(barrier, inc=1, device_id=(ep, x), device_id_type=MESH)

    own_kv = [
        pltpu.make_async_copy(ka_hbm, kv.at[z, mine, :, 0:128], kv_sem.at[0]),
        pltpu.make_async_copy(kb_hbm, kv.at[z, mine, :, 128:256], kv_sem.at[1]),
        pltpu.make_async_copy(v_hbm, kv.at[z, mine, :, 256:512], kv_sem.at[2]),
    ]
    weights = [
        pltpu.make_async_copy(wg_hbm.at[0], wg, w_sem.at[0]),
        pltpu.make_async_copy(wu_hbm.at[0], wu, w_sem.at[1]),
        pltpu.make_async_copy(wd_hbm.at[0], wd, w_sem.at[2]),
        pltpu.make_async_copy(wo_hbm, wo, w_sem.at[3]),
    ]
    for copy in own_kv + weights:
        copy.start()

    slot = lax.broadcasted_iota(jnp.int32, (EXPERTS * SLOT, TOKB), 0)
    expert, place = lax.div(slot, SLOT), lax.rem(slot, SLOT)
    first = routes[0:1, :] == expert
    second = routes[1:2, :] == expert
    member = jnp.where(first | second, 1.0, 0.0)
    earlier = lax.broadcasted_iota(jnp.int32, (TOKB, TOKB), 0) < lax.broadcasted_iota(
        jnp.int32, (TOKB, TOKB), 1
    )
    earlier = jnp.where(earlier, 1.0, 0.0).astype(BF16)
    count = jnp.dot(member.astype(BF16), earlier, preferred_element_type=F32)
    picks[...] = jnp.where(count == place.astype(F32), member, 0.0).astype(BF16)
    inputs = tok[...].astype(F32)
    scale = lax.rsqrt(jnp.mean(inputs * inputs, axis=-1, keepdims=True) + eps)
    normed[...] = (inputs * scale * gain[...]).astype(BF16)
    pl.semaphore_wait(barrier, N_EP - 1 + N_TP - 1)

    def dispatch(t, carry):
        plane = lax.rem(z + round_offset(t), Z)

        def one(q, carry):
            e = plane * PLANE + lax.rem(y + y_offset(t, q), 4) * 2 + lax.rem(q, 2)
            src = outgoing.at[e, rows]
            dst = gathered.at[t, 0, lax.div(q, 2) * 2 + core, rows]

            @pl.when(e != ep)
            def _():
                send(src, dst, disp_send, disp_recv.at[t], (e, tp))

            @pl.when(e == ep)
            def _():
                pltpu.make_async_copy(src, dst, disp_recv.at[t]).start()

            return carry

        return lax.fori_loop(0, SOURCES, one, carry)

    def pack(n):
        plane = lax.rem(z + z_offset(n), Z)
        slots = pl.ds(pl.multiple_of(plane * PLANE * SLOT, PLANE * SLOT), PLANE * SLOT)
        packed = jnp.dot(picks[slots, :], normed[...], preferred_element_type=F32)
        experts = pl.ds(plane * PLANE, PLANE)
        outgoing[experts] = packed.astype(BF16).reshape(PLANE, SLOT, D)

    def pack_and_send(n, carry):
        pack(n)
        begin = jnp.maximum(n * SPLIT - SPLIT // 2, 0)
        return lax.fori_loop(begin, n * SPLIT + SPLIT // 2, dispatch, carry)

    lax.fori_loop(0, Z, pack_and_send, 0)
    lax.fori_loop(ROUNDS - SPLIT // 2, ROUNDS, dispatch, 0)

    for copy in own_kv:
        copy.wait()

    def kv_along_z(k, carry):
        @pl.when(z + k < Z)
        def _():
            block = kv.at[z, mine]
            send(block, block, kvz_send.at[k], kvz_recv.at[k], ((z + k) * PLANE + mine, tp))

        return carry

    lax.fori_loop(1, Z, kv_along_z, 0)

    group = 2 * TOKB

    for copy in weights:
        copy.wait()

    def setup():
        first = routes[0:1, :] == lax.div(
            lax.broadcasted_iota(jnp.int32, (EXPERTS * SLOT, TOKB), 0), SLOT
        )
        weight = jnp.where(first, rweights[0:1, :], rweights[1:2, :])
        weight = jnp.transpose(picks[...].astype(F32) * weight)
        high = weight.astype(BF16)
        w_hi[...] = high
        w_lo[...] = (weight - high.astype(F32)).astype(BF16)
        returned[:, CAP:SLOT, :] = jnp.zeros((EXPERTS, SLOT - CAP, D), BF16)

        peak[...] = jnp.full_like(peak, negative)
        accum[...] = jnp.zeros_like(accum)
        lane = lax.broadcasted_iota(jnp.int32, (TOKB, 128), 1)
        for which, source in enumerate((qa, qb)):
            for g in range(2):
                pair = source[:, g * 128 : (g + 1) * 128].astype(F32) * HEAD**-0.5
                for j in range(2):
                    turned = pair if g == j else pltpu.roll(pair, 64, 1)
                    part = jnp.where((lane >= 64) == (g == 1), turned, 0.0).astype(BF16)
                    base = (which * 2 + g) * group + j * TOKB
                    qp[base : base + TOKB, which * 128 : (which + 1) * 128] = part
                    other = 1 - which
                    qp[base : base + TOKB, other * 128 : (other + 1) * 128] = jnp.zeros_like(part)

    def stage_spread(t):
        wait_for(gathered.at[t, 0, :, rows], disp_recv.at[t])
        own = gathered.at[t, 0, :, rows]
        send(own, gathered.at[t, 1, :, rows], ag1_send, ag1_recv.at[t, 0], right)
        send(own, gathered.at[t, 3, :, rows], ag1_send, ag1_recv.at[t, 1], left)

    def stage_forward(t):
        wait_for(gathered.at[t, 1, :, rows], ag1_recv.at[t, 0])
        send(
            gathered.at[t, 1, half_a, rows],
            gathered.at[t, 2, half_a, rows],
            ag2_send,
            ag2_recv.at[t, 0],
            right,
        )
        wait_for(gathered.at[t, 3, :, rows], ag1_recv.at[t, 1])
        send(
            gathered.at[t, 3, half_b, rows],
            gathered.at[t, 2, half_b, rows],
            ag2_send,
            ag2_recv.at[t, 1],
            left,
        )

    def stage_compute(t):
        wait_for(gathered.at[t, 2, half_a, rows], ag2_recv.at[t, 0])
        wait_for(gathered.at[t, 2, half_b, rows], ag2_recv.at[t, 1])
        for n in range(FFL // 256):
            cols = slice(n * 256, (n + 1) * 256)
            x = gathered[t].reshape(N_TP * SOURCES * SLOT, D)
            gate = jnp.dot(x, wg[:, cols], preferred_element_type=F32)
            up = jnp.dot(x, wu[:, cols], preferred_element_type=F32)
            capped = jnp.minimum(gate, limit_act)
            linear = jnp.clip(up, -limit_act, limit_act)
            act = capped * jax.nn.sigmoid(alpha_act * capped) * (linear + 1.0)
            hid[:, cols] = act.astype(BF16)

        def down_cols(n, carry):
            cols = pl.ds(pl.multiple_of(n * 512, 512), 512)
            part = jnp.dot(hid[...], wd[:, cols], preferred_element_type=F32)
            partial[t, :, :, :, cols] = part.astype(BF16).reshape(N_TP, SOURCES, SLOT, 512)
            return carry

        lax.fori_loop(0, D // 512, down_cols, 0)
        send(
            partial.at[t, 2, half_a, rows],
            rs1.at[t, 0, :, rows],
            rs1_send,
            rs1_recv.at[t, 0],
            right,
        )
        send(
            partial.at[t, 2, half_b, rows], rs1.at[t, 1, :, rows], rs1_send, rs1_recv.at[t, 1], left
        )
        send(
            partial.at[t, 3, half_b, rows],
            rs2.at[t, 0, half_b, rows],
            rs2_send,
            rs2_recv.at[t, 0, 1],
            right,
        )
        send(
            partial.at[t, 1, half_a, rows],
            rs2.at[t, 1, half_a, rows],
            rs2_send,
            rs2_recv.at[t, 1, 0],
            left,
        )

    def stage_add(t):
        wait_for(rs1.at[t, 0, :, rows], rs1_recv.at[t, 0])
        summed = partial[t, 3, half_a].astype(F32) + rs1[t, 0].astype(F32)
        partial[t, 3, half_a] = summed.astype(BF16)
        send(
            partial.at[t, 3, half_a, rows],
            rs2.at[t, 0, half_a, rows],
            rs2_send,
            rs2_recv.at[t, 0, 0],
            right,
        )
        wait_for(rs1.at[t, 1, :, rows], rs1_recv.at[t, 1])
        summed = partial[t, 1, half_b].astype(F32) + rs1[t, 1].astype(F32)
        partial[t, 1, half_b] = summed.astype(BF16)
        send(
            partial.at[t, 1, half_b, rows],
            rs2.at[t, 1, half_b, rows],
            rs2_send,
            rs2_recv.at[t, 1, 1],
            left,
        )

    def stage_return(t):
        for side in range(2):
            wait_for(rs2.at[t, side, half_a, rows], rs2_recv.at[t, side, 0])
            wait_for(rs2.at[t, side, half_b, rows], rs2_recv.at[t, side, 1])
        summed = partial[t, 0].astype(F32) + rs2[t, 0].astype(F32) + rs2[t, 1].astype(F32)
        back[t] = summed.astype(BF16)
        plane = lax.rem(z + Z - round_offset(t), Z)

        def one(q, carry):
            e = plane * PLANE + lax.rem(y + 4 - y_offset(t, q), 4) * 2 + lax.rem(q, 2)
            src = back.at[t, q, rows]
            dst = returned.at[ep, rows]

            @pl.when(e != ep)
            def _():
                send(src, dst, ret_send, ret_recv, (e, tp))

            @pl.when(e == ep)
            def _():
                pltpu.make_async_copy(src, dst, ret_recv).start()

            return carry

        lax.fori_loop(0, SOURCES, one, 0)

    def kv_spread(k):
        @pl.when(k > 0)
        def _():
            wait_for(kv.at[0, 0], kvz_recv.at[k])

        block = kv.at[z - k, mine]
        send(block, block, ky1_send.at[k], ky1_recv.at[k, 0], up)
        send(block, block, ky1_send.at[k], ky1_recv.at[k, 1], down)
        send(block, block, kp_send.at[k], kp_recv.at[k], peer)

    def kv_forward(k):
        near, far = pl.ds(0, TOKB // 2), pl.ds(TOKB // 2, TOKB // 2)
        block, part = kv.at[z - k, b_down], kv.at[z - k, b_down, near]
        wait_for(block, ky1_recv.at[k, 0])
        send(part, part, ky2_send.at[k], ky2_recv.at[k, 0], up)
        send(block, block, kp_send.at[k], kp_recv.at[k], peer)
        block, part = kv.at[z - k, b_up], kv.at[z - k, b_up, far]
        wait_for(block, ky1_recv.at[k, 1])
        send(part, part, ky2_send.at[k], ky2_recv.at[k, 1], down)
        send(block, block, kp_send.at[k], kp_recv.at[k], peer)

    def kv_share(k):
        block = kv.at[z - k, b_far]
        wait_for(kv.at[z - k, b_far, pl.ds(0, TOKB // 2)], ky2_recv.at[k, 0])
        wait_for(kv.at[z - k, b_far, pl.ds(TOKB // 2, TOKB // 2)], ky2_recv.at[k, 1])
        send(block, block, kp_send.at[k], kp_recv.at[k], peer)

    def visit(plane, masked):
        if masked:
            row = lax.broadcasted_iota(jnp.int32, (group, KBLOCK), 0)
            key = lax.broadcasted_iota(jnp.int32, (group, KBLOCK), 1)
            visible = key <= mine * TOKB + lax.rem(row, TOKB)
        for which in range(2):
            for g in range(2):
                at = slice((which * 2 + g) * group, (which * 2 + g + 1) * group)
                scores = lax.dot_general(
                    qp[at, :],
                    kv[plane, :, :, 0:256].reshape(KBLOCK, 256),
                    (((1,), (1,)), ((), ())),
                    preferred_element_type=F32,
                )
                if masked:
                    scores = jnp.where(visible, scores, negative)
                old = peak[at, :]
                new = jnp.maximum(old, jnp.max(scores, axis=1, keepdims=True))
                expo = jnp.exp(scores - new[:, 0:1])
                values = kv[plane, :, :, 256 + g * VDIM : 256 + (g + 1) * VDIM]
                values = values.reshape(KBLOCK, VDIM)
                values = jnp.concatenate([values, jnp.ones_like(values)], axis=1)
                mixed = jnp.dot(expo.astype(BF16), values, preferred_element_type=F32)
                fade = jnp.exp(old - new)
                accum[at, 0:VDIM] = accum[at, 0:VDIM] * fade + mixed[:, 0:VDIM]
                accum[at, VDIM:] = accum[at, VDIM:] * fade + mixed[:, VDIM:]
                peak[at, :] = new

    def kv_visit(k):
        wait_for(kv.at[0, one_core], kp_recv.at[k])

        @pl.when(k == 0)
        def _():
            visit(z, True)

        @pl.when(k > 0)
        def _():
            visit(z - k, False)

    def project():
        for g in range(2):
            for j in range(2):
                h = g * 2 + j
                a = slice(g * group + j * TOKB, g * group + (j + 1) * TOKB)
                b = slice((2 + g) * group + j * TOKB, (2 + g) * group + (j + 1) * TOKB)
                diff = accum[a, 0:VDIM] / accum[a, VDIM:] - lambdas[h] * (
                    accum[b, 0:VDIM] / accum[b, VDIM:]
                )
                scale = lax.rsqrt(jnp.mean(diff * diff, axis=-1, keepdims=True) + eps)
                heads[:, h * VDIM : (h + 1) * VDIM] = (diff * scale * head_gain[...]).astype(BF16)

        def columns(n, carry):
            cols = pl.ds(pl.multiple_of(n * 512, 512), 512)
            part = jnp.dot(heads[...], wo[:, cols], preferred_element_type=F32)
            shares[:, :, cols] = part.astype(BF16).reshape(N_TP, TOKB // N_TP, 512)
            return carry

        lax.fori_loop(0, D // 512, columns, 0)

    def mix(n, src, dst, device):
        send(src, dst, mx_send.at[n], mx_recv.at[n], device)

    def share_out():
        mix(0, shares.at[x_far, lower], passing.at[0], right)
        mix(1, shares.at[x_far, upper], passing.at[1], left)
        mix(2, shares.at[x_right, upper], arrived.at[0, upper], right)
        mix(3, shares.at[x_left, lower], arrived.at[1, lower], left)

    def relay():
        wait_for(passing.at[0], mx_recv.at[0])
        summed = shares[x_right, lower].astype(F32) + passing[0].astype(F32)
        shares[x_right, lower] = summed.astype(BF16)
        mix(4, shares.at[x_right, lower], arrived.at[0, lower], right)
        wait_for(passing.at[1], mx_recv.at[1])
        summed = shares[x_left, upper].astype(F32) + passing[1].astype(F32)
        shares[x_left, upper] = summed.astype(BF16)
        mix(5, shares.at[x_left, upper], arrived.at[1, upper], left)

    stages = (stage_spread, stage_forward, stage_compute, stage_add, stage_return)
    kv_stages = (kv_spread, kv_forward, kv_share, kv_visit)
    last_tick = ROUNDS - 1 + (len(stages) - 1) * LAG

    def tick(i, carry):
        for n in range(len(stages)):
            t = i - n * LAG

            @pl.when((t >= 0) & (t < ROUNDS))
            def _(n=n, t=t):
                stages[n](t)

        for n in range(len(kv_stages)):
            step = i - KV_LAG
            k = lax.div(step, KV_STEP) - n

            @pl.when((step >= 0) & (lax.rem(step, KV_STEP) == 0) & (k >= 0) & (k < Z) & (k <= z))
            def _(n=n, k=k):
                kv_stages[n](k)

        @pl.when(i == SETUP_TICK)
        def _():
            setup()

        @pl.when(i == KV_LAG + (Z + len(kv_stages) - 1) * KV_STEP)
        def _():
            project()

        @pl.when(i == last_tick - LAG)
        def _():
            share_out()

        @pl.when(i == last_tick)
        def _():
            relay()

        return carry

    lax.fori_loop(0, last_tick + 1, tick, 0)

    wait_for(returned.at[:, rows], ret_recv)

    def combine(n, carry):
        cols = pl.ds(pl.multiple_of(n * 512, 512), 512)
        table = returned[:, :, cols].reshape(EXPERTS * SLOT, 512)
        total = jnp.dot(w_hi[...], table, preferred_element_type=F32)
        total = total + jnp.dot(w_lo[...], table, preferred_element_type=F32)
        out[:, cols] = total.astype(BF16)
        return carry

    lax.fori_loop(0, D // 512, combine, 0)

    total = shares[tp].astype(F32)
    for n in range(2, 6):
        wait_for(passing.at[0], mx_recv.at[n])
    total = total + arrived[0].astype(F32) + arrived[1].astype(F32)
    mixer[...] = total.astype(BF16)

    some = pl.ds(0, N_EP - 1)
    wait_for(outgoing.at[some, rows], disp_send)
    wait_for(returned.at[some, rows], ret_send)
    wait_for(gathered.at[:, 0:2, :, rows], ag1_send)
    wait_for(back.at[:, :, rows], ag2_send)
    wait_for(back.at[:, :, rows], rs1_send)
    wait_for(gathered.at[:, 0:2, :, rows], rs2_send)
    for n in range(6):
        wait_for(passing.at[0], mx_send.at[n])

    def kv_sent(k, carry):
        @pl.when((k > 0) & (z + k < Z))
        def _():
            wait_for(kv.at[0, 0], kvz_send.at[k])

        @pl.when(k <= z)
        def _():
            wait_for(kv.at[0, 0:2], ky1_send.at[k])
            wait_for(kv.at[0, 0], ky2_send.at[k])
            wait_for(kv.at[0, one_core], kp_send.at[k])

        return carry

    lax.fori_loop(0, Z, kv_sent, 0)


def body(
    queries_a,
    queries_b,
    keys_a,
    keys_b,
    values,
    lambdas,
    head_gain,
    w_out,
    moe_tokens,
    moe_gain,
    routes,
    route_weights,
    w_gate,
    w_up,
    w_down,
):
    dma = pltpu.SemaphoreType.DMA
    vmem = pl.BlockSpec(memory_space=pltpu.VMEM)
    hbm = pl.BlockSpec(memory_space=pl.ANY)
    moe_out, mixer_out = pl.pallas_call(
        kernel,
        out_shape=(
            jax.ShapeDtypeStruct((TOKB, D), BF16),
            jax.ShapeDtypeStruct((TOKB // N_TP, D), BF16),
        ),
        in_specs=[vmem] * 6 + [pl.BlockSpec(memory_space=pltpu.SMEM), vmem] + [hbm] * 7,
        out_specs=(vmem, vmem),
        scratch_shapes=[
            pltpu.VMEM((D, FFL), BF16),
            pltpu.VMEM((D, FFL), BF16),
            pltpu.VMEM((FFL, D), BF16),
            pltpu.VMEM((EXPERTS * SLOT, TOKB), BF16),
            pltpu.VMEM((TOKB, D), BF16),
            pltpu.VMEM((EXPERTS, SLOT, D), BF16),
            pltpu.VMEM((ROUNDS, N_TP, SOURCES, SLOT, D), BF16),
            pltpu.VMEM((ROUNDS, N_TP, SOURCES, SLOT, D), BF16),
            pltpu.VMEM((ROUNDS, 2, SOURCES // 2, SLOT, D), BF16),
            pltpu.VMEM((ROUNDS, 2, SOURCES, SLOT, D), BF16),
            pltpu.VMEM((ROUNDS, SOURCES, SLOT, D), BF16),
            pltpu.VMEM((EXPERTS, SLOT, D), BF16),
            pltpu.VMEM((N_TP * SOURCES * SLOT, FFL), BF16),
            pltpu.VMEM((TOKB, EXPERTS * SLOT), BF16),
            pltpu.VMEM((TOKB, EXPERTS * SLOT), BF16),
            pltpu.VMEM((Z, PLANE, TOKB, 512), BF16),
            pltpu.VMEM((512, D), BF16),
            pltpu.VMEM((8 * TOKB, 256), BF16),
            pltpu.VMEM((8 * TOKB, 128), F32),
            pltpu.VMEM((8 * TOKB, 256), F32),
            pltpu.VMEM((TOKB, 512), BF16),
            pltpu.VMEM((N_TP, TOKB // N_TP, D), BF16),
            pltpu.VMEM((2, TOKB // N_TP // 2, D), BF16),
            pltpu.VMEM((2, TOKB // N_TP, D), BF16),
            dma((4,)),
            dma((3,)),
            dma,
            dma((ROUNDS,)),
            dma,
            dma((ROUNDS, 2)),
            dma,
            dma((ROUNDS, 2)),
            dma,
            dma((ROUNDS, 2)),
            dma,
            dma((ROUNDS, 2, 2)),
            dma,
            dma,
            dma((Z,)),
            dma((Z,)),
            dma((Z,)),
            dma((Z, 2)),
            dma((Z,)),
            dma((Z, 2)),
            dma((Z,)),
            dma((Z,)),
            dma((6,)),
            dma((6,)),
        ],
        compiler_params=pltpu.CompilerParams(
            collective_id=0, has_side_effects=True, vmem_limit_bytes=60 * 1024 * 1024
        ),
        name="layer",
    )(
        moe_tokens,
        moe_gain.reshape(1, D),
        routes.T,
        route_weights.T,
        queries_a,
        queries_b,
        lambdas,
        head_gain.reshape(1, VDIM),
        keys_a,
        keys_b,
        values,
        w_out,
        w_gate,
        w_up,
        w_down,
    )
    return (mixer_out, moe_out)


def solution(mesh):
    return jax.shard_map(
        body,
        mesh=mesh,
        in_specs=(
            P("ep", "tp"),
            P("ep", "tp"),
            P("ep", "tp"),
            P("ep", "tp"),
            P("ep", "tp"),
            P("tp"),
            P(),
            P("tp", None),
            P(("ep", "tp"), None),
            P(),
            P(("ep", "tp"), None),
            P(("ep", "tp"), None),
            P("ep", None, "tp"),
            P("ep", None, "tp"),
            P("ep", "tp", None),
        ),
        out_specs=(P(("ep", "tp"), None), P(("ep", "tp"), None)),
        check_vma=False,
    )
```
